32 devices in a mesh: sp: 4 (over y, x), dp: 8 (over z, core).
Axes of the slice: x: 2, y: 2, z: 4, core: 2. Of those that a mesh axis runs over, the one named last changes fastest.
Arguments:
- tokens: bfloat16 [8, 1024, 2048], P('dp', 'sp'), may hold values from -6 to 6
- key_weight: bfloat16 [2048, 2048], P('dp'), may hold values from -0.125 to 0.125
- queries: bfloat16 [8, 1024, 16, 128], P('dp', None, 'sp'), may hold values from -1.5 to 1.5
- values: bfloat16 [8, 1024, 16, 256], P('dp', None, 'sp'), may hold values from -1.5 to 1.5
- cotangent: bfloat16 [8, 1024, 4096], P('dp', 'sp'), may hold values from -6 to 6
- log_decay: float32 [16], replicated, may hold values from -0.034 to 0, as said below
Outputs:
- grad_tokens: bfloat16 [8, 1024, 2048], P('dp', 'sp')
- grad_queries: bfloat16 [8, 1024, 16, 128], P('dp', None, 'sp')
- grad_values: bfloat16 [8, 1024, 16, 256], P('dp', None, 'sp')
- grad_key_weight: float32 [2048, 2048], P('dp')
The draws below stay inside these ranges and needn't reach their ends.
Inputs may be any that keep to these rules, and one draw needn't show every extreme that they name: `log_decay`: every entry is below zero.
All inputs are finite; a program needn't handle non-finite values.
Results may differ from the reference program's by a relative error of at most 0.0075.
Values may be sent and summed in bfloat16 or wider, within the bound.
No kernel may reach another device: no remote copies, remote signals or barrier semaphores. Data moves between devices by JAX's collectives and lax.ppermute only.
A program may use at most 128 MiB of HBM per device.

```python
import jax
import jax.numpy as jnp
from jax import lax

D = 2048
HEADS = 16
KEY_DIM = 128
VALUE_DIM = 256
BLOCK = 128
LENGTH = 1024
SEQS = 8


def draw_log_decay(key, part):
    ranking = jax.random.permutation(jax.random.fold_in(key, 11), HEADS)
    fast_count = HEADS // 2
    spread = jax.random.uniform(jax.random.fold_in(key, 12), (HEADS,), jnp.float32)
    slow_rate = jnp.minimum(jnp.exp(jnp.log(0.2 / LENGTH) + spread * jnp.log(10.0)), 0.01)
    fast_rate = jnp.exp(jnp.log(0.01) + spread * jnp.log(100.0 / 30.0))
    return -jnp.where(ranking < fast_count, fast_rate, slow_rate).astype(jnp.float32)


def raised(result, rng, source, target, shards_of, factor):
    def block_of(dim):
        return (jnp.arange(result.shape[dim]) // (result.shape[dim] // shards_of)).reshape((-1,) + (1,) * (result.ndim - 1 - dim))

    first = jax.random.permutation(rng, shards_of)[block_of(target)]
    second = (block_of(target) + shards_of // 2) % shards_of
    return jnp.where((block_of(source) == first) | (block_of(source) == second), factor * result, result)


def block_scale(own_key, shape, shards, smallest, high):
    gain, own = 1.0, jax.random.fold_in(own_key, 6)
    for axis_at, shards_of in shards:
        heights = jnp.exp(jax.random.uniform(jax.random.fold_in(own, axis_at), (shards_of,), jnp.float32, smallest / len(shards), high / len(shards)))
        gain = gain * jnp.repeat(heights, shape[axis_at] // shards_of).reshape([-1 if axis == axis_at else 1 for axis in range(len(shape))])
    return gain


def gaussian(key, shape, scale, reach, pieces=(), kind=jnp.bfloat16):
    factor_of = block_scale(key, shape, pieces, -0.22, 0.18) if pieces else 1.0
    result = jax.random.normal(key, shape, jnp.float32) * scale * factor_of
    return jnp.minimum(jnp.maximum(result, -reach), reach).astype(kind)


def bell_draw_with(stream_key, extent, deviation, bound, pieces, heavy, kind=jnp.bfloat16):
    result = deviation * jax.random.normal(stream_key, extent, jnp.float32)
    if pieces:
        result = result * block_scale(stream_key, extent, pieces, -0.22, 0.18)
    return jnp.clip(raised(result, jax.random.fold_in(stream_key, 3), *heavy), -bound, bound).astype(kind)


def setup_inputs(seed: int = 0) -> dict:
    arg_keys = jax.random.split(jax.random.key(seed), 7)
    tokens = gaussian(arg_keys[0], (SEQS, LENGTH, D), 1.0, 6.0, ((0, 8), (1, 4)))
    key_weight = gaussian(arg_keys[1], (HEADS * KEY_DIM, D), D ** -0.5, 0.125, ((0, 8),))
    queries = gaussian(arg_keys[2], (SEQS, LENGTH, HEADS, KEY_DIM), 0.1, 1.5, ((0, 8), (2, 4)))
    values = gaussian(arg_keys[3], (SEQS, LENGTH, HEADS, VALUE_DIM), 0.1, 1.5, ((0, 8), (2, 4)))
    cotangent = bell_draw_with(arg_keys[4], (SEQS, LENGTH, HEADS * VALUE_DIM), 1.0, 6.0, ((0, 8), (1, 4)), (0, 2, 8, 2.0))
    log_decay = draw_log_decay(jax.random.fold_in(arg_keys[6], 71), 0)
    return {"tokens": tokens, "key_weight": key_weight, "queries": queries, "values": values, "cotangent": cotangent, "log_decay": log_decay}


def product(form, left, right):
    return jnp.einsum(form, left.astype(jnp.float32), right.astype(jnp.float32))


def rotation(seq_len, half):
    position = jnp.arange(seq_len, dtype=jnp.float32)
    frequency = 10000.0 ** (-jnp.arange(half, dtype=jnp.float32) / half)
    angle = position[:, None] * frequency[None, :]
    return jnp.cos(angle)[:, None, :], jnp.sin(angle)[:, None, :]


def rotate(vectors, cosine, sine):
    half = vectors.shape[-1] // 2
    front, back = vectors[..., :half], vectors[..., half:]
    return jnp.concatenate([front * cosine - back * sine, front * sine + back * cosine], axis=-1)


def unrotate(grads, cosine, sine):
    half = grads.shape[-1] // 2
    front, back = grads[..., :half], grads[..., half:]
    return jnp.concatenate([front * cosine + back * sine, back * cosine - front * sine], axis=-1)


def retention_backward(query_rows, key_rows, value_rows, cotan_rows, head_decay):
    seq_len, heads_here, key_width = query_rows.shape
    nblocks = seq_len // BLOCK
    cosine, sine = rotation(seq_len, key_width // 2)
    factor = key_width ** -0.5
    rot_query = rotate(query_rows.astype(jnp.float32), cosine, sine).astype(jnp.bfloat16)
    rot_key = (rotate(key_rows.astype(jnp.float32), cosine, sine) * factor).astype(jnp.bfloat16)

    def blocks(array):
        return array.reshape(nblocks, BLOCK, heads_here, array.shape[-1])

    block_query, block_key = blocks(rot_query), blocks(rot_key)
    block_value, block_cotan = blocks(value_rows), blocks(cotan_rows)
    inside = jnp.arange(BLOCK, dtype=jnp.float32)
    offset = inside[:, None] - inside[None, :]
    within = jnp.where(offset[None] >= 0, jnp.exp(jnp.maximum(offset, 0.0)[None] * head_decay[:, None, None]), 0.0)
    rising = jnp.exp((inside + 1.0)[:, None] * head_decay[None, :])[None, :, :, None]
    falling = jnp.exp((BLOCK - 1.0 - inside)[:, None] * head_decay[None, :])[None, :, :, None]
    scores = (product("nihd,njhd->nhij", block_query, block_key) * within[None]).astype(jnp.bfloat16)
    mixing = (product("nihe,njhe->nhij", block_cotan, block_value) * within[None]).astype(jnp.bfloat16)
    decayed_queries = (block_query.astype(jnp.float32) * rising).astype(jnp.bfloat16)
    decayed_keys = (block_key.astype(jnp.float32) * falling).astype(jnp.bfloat16)
    block_states = product("nihd,nihe->nhde", decayed_keys, block_value)
    block_trails = product("nihd,nihe->nhde", decayed_queries, block_cotan)
    block_index = jnp.arange(nblocks, dtype=jnp.float32)
    spacing = block_index[:, None] - block_index[None, :] - 1.0
    earlier = jnp.where(spacing[None] >= 0,
                        jnp.exp(jnp.maximum(spacing, 0.0)[None] * BLOCK * head_decay[:, None, None]), 0.0)
    later = jnp.transpose(earlier, (0, 2, 1))
    entering = jnp.einsum("hnm,mhde->nhde", earlier, block_states,
                          precision=lax.Precision.HIGHEST).astype(jnp.bfloat16)
    trailing = jnp.einsum("hnm,mhde->nhde", later, block_trails,
                          precision=lax.Precision.HIGHEST).astype(jnp.bfloat16)
    grad_rq = product("nhij,njhd->nihd", mixing, block_key) + rising * product("nihe,nhde->nihd", block_cotan, entering)
    grad_rk = product("nhij,nihd->njhd", mixing, block_query) + falling * product("nihe,nhde->nihd", block_value, trailing)
    grad_value = product("nhij,nihe->njhe", scores, block_cotan) + falling * product("nihd,nhde->nihe", block_key, trailing)
    grad_rq = grad_rq.reshape(seq_len, heads_here, key_width)
    grad_rk = grad_rk.reshape(seq_len, heads_here, key_width)
    grad_query = unrotate(grad_rq, cosine, sine).astype(jnp.bfloat16)
    grad_key = (unrotate(grad_rk, cosine, sine) * factor).astype(jnp.bfloat16)
    grad_value = grad_value.reshape(seq_len, heads_here, -1).astype(jnp.bfloat16)
    return grad_query, grad_key, grad_value


def reference(tokens, key_weight, queries, values, cotangent, log_decay):
    seq_len = tokens.shape[1]

    def one_sequence(weight_sum, item):
        token_rows, query_rows, value_rows, cotan_rows = item
        key_proj = jnp.dot(token_rows, key_weight.T, preferred_element_type=jnp.float32).astype(jnp.bfloat16)
        grad_query, grad_key, grad_value = retention_backward(
            query_rows, key_proj.reshape(seq_len, HEADS, KEY_DIM), value_rows,
            cotan_rows.reshape(seq_len, HEADS, VALUE_DIM), log_decay)
        key_grads = grad_key.reshape(seq_len, HEADS * KEY_DIM)
        grad_token = jnp.dot(key_grads, key_weight, preferred_element_type=jnp.float32).astype(jnp.bfloat16)
        weight_sum = weight_sum + jnp.dot(key_grads.T, token_rows, preferred_element_type=jnp.float32)
        return weight_sum, (grad_token, grad_query, grad_value)

    start_sum = jnp.zeros((HEADS * KEY_DIM, D), jnp.float32)
    weight_grad, outputs = lax.scan(one_sequence, start_sum, (tokens, queries, values, cotangent))
    return outputs[0], outputs[1], outputs[2], weight_grad
```

```python
import jax
import jax.numpy as jnp
from jax import lax
from jax.experimental import pallas as pl
from jax.experimental.pallas import tpu as pltpu
from jax.sharding import PartitionSpec as P

BLOCK = 128


def product(form, left, right):
    return jnp.einsum(form, left, right, preferred_element_type=jnp.float32)


def rotation(seq_len, half):
    position = jnp.arange(seq_len, dtype=jnp.float32)
    frequency = 10000.0 ** (-jnp.arange(half, dtype=jnp.float32) / half)
    angle = position[:, None] * frequency[None, :]
    return (jnp.cos(angle)[:, None, :], jnp.sin(angle)[:, None, :])


def rotate(vectors, cosine, sine):
    half = vectors.shape[-1] // 2
    front, back = (vectors[..., :half], vectors[..., half:])
    return jnp.concatenate([front * cosine - back * sine, front * sine + back * cosine], axis=-1)


def unrotate(grads, cosine, sine):
    half = grads.shape[-1] // 2
    front, back = (grads[..., :half], grads[..., half:])
    return jnp.concatenate([front * cosine + back * sine, back * cosine - front * sine], axis=-1)


def retention_backward(query_rows, key_rows, value_rows, cotan_rows, head_decay):
    seq_len, heads_here, key_width = query_rows.shape
    nblocks = seq_len // BLOCK
    cosine, sine = rotation(seq_len, key_width // 2)
    factor = key_width ** (-0.5)
    rot_query = rotate(query_rows.astype(jnp.float32), cosine, sine).astype(jnp.bfloat16)
    rot_key = (rotate(key_rows.astype(jnp.float32), cosine, sine) * factor).astype(jnp.bfloat16)

    def blocks(array):
        return array.reshape(nblocks, BLOCK, heads_here, array.shape[-1])

    block_query, block_key = (blocks(rot_query), blocks(rot_key))
    block_value, block_cotan = (blocks(value_rows), blocks(cotan_rows))
    inside = jnp.arange(BLOCK, dtype=jnp.float32)
    offset = inside[:, None] - inside[None, :]
    within = jnp.where(
        offset[None] >= 0, jnp.exp(jnp.maximum(offset, 0.0)[None] * head_decay[:, None, None]), 0.0
    )
    rising = jnp.exp((inside + 1.0)[:, None] * head_decay[None, :])[None, :, :, None]
    falling = jnp.exp((BLOCK - 1.0 - inside)[:, None] * head_decay[None, :])[None, :, :, None]
    scores = (product("nihd,njhd->nhij", block_query, block_key) * within[None]).astype(
        jnp.bfloat16
    )
    mixing = (product("nihe,njhe->nhij", block_cotan, block_value) * within[None]).astype(
        jnp.bfloat16
    )
    decayed_queries = (block_query.astype(jnp.float32) * rising).astype(jnp.bfloat16)
    decayed_keys = (block_key.astype(jnp.float32) * falling).astype(jnp.bfloat16)
    block_states = product("nihd,nihe->nhde", decayed_keys, block_value)
    block_trails = product("nihd,nihe->nhde", decayed_queries, block_cotan)
    block_index = jnp.arange(nblocks, dtype=jnp.float32)
    spacing = block_index[:, None] - block_index[None, :] - 1.0
    earlier = jnp.where(
        spacing[None] >= 0,
        jnp.exp(jnp.maximum(spacing, 0.0)[None] * BLOCK * head_decay[:, None, None]),
        0.0,
    )
    later = jnp.transpose(earlier, (0, 2, 1))
    entering = jnp.einsum(
        "hnm,mhde->nhde", earlier, block_states, precision=lax.Precision.HIGHEST
    ).astype(jnp.bfloat16)
    trailing = jnp.einsum(
        "hnm,mhde->nhde", later, block_trails, precision=lax.Precision.HIGHEST
    ).astype(jnp.bfloat16)
    grad_rq = product("nhij,njhd->nihd", mixing, block_key) + rising * product(
        "nihe,nhde->nihd", block_cotan, entering
    )
    grad_rk = product("nhij,nihd->njhd", mixing, block_query) + falling * product(
        "nihe,nhde->nihd", block_value, trailing
    )
    grad_value = product("nhij,nihe->njhe", scores, block_cotan) + falling * product(
        "nihd,nhde->nihe", block_key, trailing
    )
    grad_rq = grad_rq.reshape(seq_len, heads_here, key_width)
    grad_rk = grad_rk.reshape(seq_len, heads_here, key_width)
    grad_query = unrotate(grad_rq, cosine, sine).astype(jnp.bfloat16)
    grad_key = (unrotate(grad_rk, cosine, sine) * factor).astype(jnp.bfloat16)
    grad_value = grad_value.reshape(seq_len, heads_here, -1).astype(jnp.bfloat16)
    return (grad_query, grad_key, grad_value)


def general_body(tokens, key_weight, queries, values, cotangent, log_decay):
    gathered = lax.all_gather(key_weight, "dp", axis=0, tiled=True)
    token_rows = tokens[0]
    key_proj = jnp.einsum(
        "td,qd->tq", token_rows, gathered, preferred_element_type=jnp.float32
    ).astype(jnp.bfloat16)
    head_keys, head_cotan = (
        lax.all_to_all(key_proj[None], "sp", split_axis=2, concat_axis=1, tiled=True),
        lax.all_to_all(cotangent, "sp", split_axis=2, concat_axis=1, tiled=True),
    )
    seq_len = head_keys.shape[1]
    heads_here = queries.shape[2]
    head_start = lax.axis_index("sp") * heads_here
    head_decay = lax.dynamic_slice_in_dim(log_decay, head_start, heads_here)
    grad_query, grad_key, grad_value = retention_backward(
        queries[0],
        head_keys[0].reshape(seq_len, heads_here, -1),
        values[0],
        head_cotan[0].reshape(seq_len, heads_here, -1),
        head_decay,
    )
    returned = lax.all_to_all(
        grad_key.reshape(1, seq_len, -1), "sp", split_axis=1, concat_axis=2, tiled=True
    )
    key_grads = returned[0]
    grad_tokens = jnp.dot(key_grads, gathered, preferred_element_type=jnp.float32).astype(
        jnp.bfloat16
    )
    width = key_grads.shape[1]
    count_dp = lax.axis_size("dp")
    count_sp = lax.axis_size("sp")
    share = width // (count_sp * count_dp)
    ordered = (
        key_grads.reshape(-1, count_dp, count_sp, share).transpose(0, 2, 1, 3).reshape(-1, width)
    )
    partial_grad = jnp.einsum("tq,td->qd", ordered, token_rows, preferred_element_type=jnp.float32)
    owned = lax.psum_scatter(partial_grad, ("sp", "dp"), scatter_dimension=0, tiled=True)
    weight_grad = lax.all_gather(owned, "sp", axis=0, tiled=True)
    return (grad_tokens[None], grad_query[None], grad_value[None], weight_grad)


INNER = 256


def swap(array, axis, bit):
    count = lax.axis_size(axis)
    return lax.ppermute(array, axis, [(i, i ^ bit) for i in range(count)])


def step_planes(array):
    count = lax.axis_size("dp")
    return lax.ppermute(array, "dp", [(i, (i + 2) % count) for i in range(count)])


def dot(left, right, left_dim, right_dim):
    return lax.dot_general(
        left, right, (((left_dim,), (right_dim,)), ((), ())), preferred_element_type=jnp.float32
    )


def columns(array, index, width):
    return lax.dynamic_slice_in_dim(array, index * width, width, axis=1)


def cost(flops, moved):
    return pl.CostEstimate(flops=int(flops), bytes_accessed=int(moved), transcendentals=0)


def spec(shape, index):
    return pl.BlockSpec(shape, index)


def decays(rate, size):
    rows = lax.broadcasted_iota(jnp.int32, (size, size), 0)
    cols = lax.broadcasted_iota(jnp.int32, (size, size), 1)
    gap = (rows - cols).astype(jnp.float32)
    within = jnp.where(gap >= 0, jnp.exp(jnp.maximum(gap, 0.0) * rate), 0.0)
    place = lax.broadcasted_iota(jnp.int32, (size, 1), 0).astype(jnp.float32)
    rising = jnp.exp((place + 1.0) * rate)
    falling = jnp.exp((size - 1.0 - place) * rate)
    whole = jnp.exp(jnp.full((1, 1), float(size), jnp.float32) * rate)
    return within, rising, falling, whole


def turn(block, cosine, sine):
    half = block.shape[-1] // 2
    return block * cosine + pltpu.roll(block, half, 1) * sine


def turn_back(block, cosine, sine):
    half = block.shape[-1] // 2
    return block * cosine - pltpu.roll(block, half, 1) * sine


def first_kernel(slots, rows, inner, factor):
    def kernel(*refs):
        place, rate_ref, query, value, cosine, sine = refs[:6]
        cotans = refs[6 : 6 + slots]
        outs = refs[6 + slots :]
        grads, rotated, mixing, trailing, cotan, whole_grad = (
            outs[:slots],
            outs[slots],
            outs[slots + 1],
            outs[slots + 2],
            outs[slots + 3],
            outs[slots + 4],
        )
        here = place[0]
        rate = rate_ref[pl.program_id(0)]
        for k in range(slots):
            cotan[pl.ds((here ^ k) * rows, rows), :] = cotans[k][...]
        within, rising, falling, whole = decays(rate, inner)
        seq_len = query.shape[0]
        carry = jnp.zeros((query.shape[1], value.shape[1]), jnp.float32)
        for n in reversed(range(seq_len // inner)):
            at = slice(n * inner, (n + 1) * inner)
            cos, sin = cosine[at, :], sine[at, :]
            turned = turn(query[at, :].astype(jnp.float32), cos, sin).astype(jnp.bfloat16)
            rotated[at, :] = turned
            co, va = cotan[at, :], value[at, :]
            mix = (dot(co, va, 1, 1) * within).astype(jnp.bfloat16)
            mixing[0, n] = mix
            trail = carry.astype(jnp.bfloat16)
            trailing[0, n] = trail
            grad = dot(mix, turned, 0, 0) + falling * dot(va, trail, 1, 1)
            grad = turn_back(grad, cos, sin) * factor
            whole_grad[at, :] = grad.astype(jnp.bfloat16)
            decayed = (turned.astype(jnp.float32) * rising).astype(jnp.bfloat16)
            carry = carry * whole + dot(decayed, co, 0, 0)
        for k in range(slots):
            grads[k][...] = whole_grad[pl.ds((here ^ k) * rows, rows), :]

    return kernel


def second_kernel(slots, rows, inner, factor):
    def kernel(*refs):
        place, rate_ref, rotated, value, cosine, sine, mixing, trailing, keys = refs[:9]
        cotans = refs[9 : 9 + slots]
        grad_query, grad_value, cotan, key = refs[9 + slots :]
        here = place[0]
        rate = rate_ref[pl.program_id(0)]
        for k in range(slots):
            at = pl.ds((here ^ k) * rows, rows)
            cotan[at, :] = cotans[k][...]
            key[at, :] = keys[k]
        within, rising, falling, whole = decays(rate, inner)
        seq_len = rotated.shape[0]
        carry = jnp.zeros((rotated.shape[1], value.shape[1]), jnp.float32)
        for n in range(seq_len // inner):
            at = slice(n * inner, (n + 1) * inner)
            cos, sin = cosine[at, :], sine[at, :]
            rk = (turn(key[at, :].astype(jnp.float32), cos, sin) * factor).astype(jnp.bfloat16)
            rq, co, va = rotated[at, :], cotan[at, :], value[at, :]
            score = (dot(rq, rk, 1, 1) * within).astype(jnp.bfloat16)
            entering = carry.astype(jnp.bfloat16)
            grad = dot(mixing[0, n], rk, 1, 0) + rising * dot(co, entering, 1, 1)
            grad_query[at, :] = turn_back(grad, cos, sin).astype(jnp.bfloat16)
            grad_value[at, :] = (
                dot(score, co, 0, 0) + falling * dot(rk, trailing[0, n], 1, 0)
            ).astype(jnp.bfloat16)
            decayed = (rk.astype(jnp.float32) * falling).astype(jnp.bfloat16)
            carry = carry * whole + dot(decayed, va, 0, 0)

    return kernel


def prefetch(*values):
    return jnp.stack([jnp.asarray(v, jnp.int32) for v in values])


def smem():
    return pl.BlockSpec(memory_space=pltpu.SMEM)


def retention_first(here, rate, query, value, cosine, sine, cotans, key_width):
    slots = len(cotans)
    seq_len, query_width = query.shape
    heads = query_width // key_width
    value_width = value.shape[1] // heads
    rows = cotans[0].shape[0]
    inner = min(INNER, rows)
    nblocks = seq_len // inner
    half = jnp.bfloat16
    full = spec((seq_len, key_width), lambda h: (0, 0))
    head = spec((seq_len, key_width), lambda h: (0, h))
    outs = [jax.ShapeDtypeStruct((rows, query_width), half)] * slots + [
        jax.ShapeDtypeStruct((seq_len, query_width), half),
        jax.ShapeDtypeStruct((heads, nblocks, inner, inner), half),
        jax.ShapeDtypeStruct((heads, nblocks, key_width, value_width), half),
    ]
    result = pl.pallas_call(
        first_kernel(slots, rows, inner, key_width**-0.5),
        grid=(heads,),
        in_specs=[smem(), smem(), head, spec((seq_len, value_width), lambda h: (0, h)), full, full]
        + [spec((rows, value_width), lambda h: (0, h))] * slots,
        out_specs=[spec((rows, key_width), lambda h: (0, h))] * slots
        + [
            head,
            spec((1, nblocks, inner, inner), lambda h: (h, 0, 0, 0)),
            spec((1, nblocks, key_width, value_width), lambda h: (h, 0, 0, 0)),
        ],
        out_shape=outs,
        scratch_shapes=[
            pltpu.VMEM((seq_len, value_width), half),
            pltpu.VMEM((seq_len, key_width), half),
        ],
        cost_estimate=cost(4e9, 10e6),
        name="retention_first",
    )(prefetch(here), rate, query, value, cosine, sine, *cotans)
    return list(result[:slots]), result[slots], result[slots + 1], result[slots + 2]


def retention_second(here, rate, rotated, value, cosine, sine, mixing, trailing, keys, cotans):
    slots = len(cotans)
    heads, nblocks, key_width, value_width = trailing.shape
    inner = mixing.shape[-1]
    seq_len = rotated.shape[0]
    rows = cotans[0].shape[0]
    half = jnp.bfloat16
    full = spec((seq_len, key_width), lambda h: (0, 0))
    head = spec((seq_len, key_width), lambda h: (0, h))
    wide = spec((seq_len, value_width), lambda h: (0, h))
    return pl.pallas_call(
        second_kernel(slots, rows, inner, key_width**-0.5),
        grid=(heads,),
        in_specs=[
            smem(),
            smem(),
            head,
            wide,
            full,
            full,
            spec((1, nblocks, inner, inner), lambda h: (h, 0, 0, 0)),
            spec((1, nblocks, key_width, value_width), lambda h: (h, 0, 0, 0)),
            spec((slots, rows, key_width), lambda h: (0, 0, h)),
        ]
        + [spec((rows, value_width), lambda h: (0, h))] * slots,
        out_specs=[head, wide],
        out_shape=[
            jax.ShapeDtypeStruct(rotated.shape, half),
            jax.ShapeDtypeStruct(value.shape, half),
        ],
        scratch_shapes=[
            pltpu.VMEM((seq_len, value_width), half),
            pltpu.VMEM((seq_len, key_width), half),
        ],
        cost_estimate=cost(4e9, 14e6),
        name="retention_second",
    )(prefetch(here), rate, rotated, value, cosine, sine, mixing, trailing, keys, *cotans)


def key_projection(here, plane, core, tokens, shards):
    slots = len(tokens)
    planes = len(shards)
    rows, width = tokens[0].shape
    share = shards[0][0].shape[0]

    def kernel(*refs):
        place = refs[0]
        token_refs = refs[1 : 1 + slots]
        shard_refs = refs[1 + slots : 1 + slots + 2 * planes]
        out, weight, sems = refs[1 + slots + 2 * planes :]
        slot, own = place[0], place[1]

        @pl.when(pl.program_id(0) == 0)
        def _():
            for r in range(planes):

                @pl.when(slot == r)
                def _():
                    for side in range(2):
                        pltpu.make_async_copy(
                            shard_refs[2 * r + side], weight.at[own ^ side], sems.at[side]
                        ).start()

            for side in range(2):
                pltpu.make_async_copy(
                    shard_refs[side], weight.at[own ^ side], sems.at[side]
                ).wait()

        for k in range(slots):

            @pl.when(pl.program_id(0) == k)
            def _():
                for side in range(2):
                    out[0, :, side * share : (side + 1) * share] = dot(
                        token_refs[k][...], weight[side], 1, 1
                    ).astype(jnp.bfloat16)

    whole = spec((rows, width), lambda k: (0, 0))
    anywhere = pl.BlockSpec(memory_space=pl.ANY)
    return pl.pallas_call(
        kernel,
        grid=(slots,),
        in_specs=[smem()] + [whole] * slots + [anywhere] * (2 * planes),
        out_specs=spec((1, rows, 2 * share), lambda k: (k, 0, 0)),
        out_shape=jax.ShapeDtypeStruct((slots, rows, 2 * share), jnp.bfloat16),
        scratch_shapes=[
            pltpu.VMEM((2, share, width), jnp.bfloat16),
            pltpu.SemaphoreType.DMA((2,)),
        ],
        cost_estimate=cost(2.2e9, 8e6),
        name="key_projection",
    )(
        prefetch((plane - here) % planes, core),
        *tokens,
        *[part for pair in shards for part in pair],
    )


def token_gradient(here, plane, core, grads, shards):
    slots = len(grads)
    planes = len(shards)
    rows = grads[0].shape[0]
    share, width = shards[0][0].shape
    tile = width // 4

    def kernel(*refs):
        place = refs[0]
        grad_refs = refs[1 : 1 + slots]
        shard_refs = refs[1 + slots : 1 + slots + 2 * planes]
        out, stack = refs[1 + slots + 2 * planes :]
        own = place[2]

        @pl.when(pl.program_id(0) == 0)
        def _():
            for k in range(slots):
                low, high = grad_refs[k][:, :share], grad_refs[k][:, share:]
                stack[k, 0] = jnp.where(own == 0, low, high)
                stack[k, 1] = jnp.where(own == 0, high, low)

        total = jnp.zeros((rows, tile), jnp.float32)
        for r in range(planes):
            k = ((place[1] + planes - r) % planes) ^ place[0]
            for side in range(2):
                total += dot(stack[k, side], shard_refs[2 * r + side][...], 1, 0)
        out[...] = total.astype(jnp.bfloat16)

    return pl.pallas_call(
        kernel,
        grid=(width // tile,),
        in_specs=[smem()]
        + [spec((rows, 2 * share), lambda m: (0, 0))] * slots
        + [spec((share, tile), lambda m: (0, m))] * (2 * planes),
        out_specs=spec((rows, tile), lambda m: (0, m)),
        out_shape=jax.ShapeDtypeStruct((rows, width), jnp.bfloat16),
        scratch_shapes=[pltpu.VMEM((slots, 2, rows, share), jnp.bfloat16)],
        cost_estimate=cost(2.2e9, 11e6),
        name="token_gradient",
    )(prefetch(here, plane, core), *grads, *[part for pair in shards for part in pair])


def weight_partial(core, grads, tokens, flip):
    slots = len(grads)
    rows, width = tokens[0].shape
    share = grads[0].shape[1] // 2
    tile = width // 4

    def kernel(*refs):
        grad_refs, token_refs, out = refs[1 : 1 + slots], refs[1 + slots : 1 + 2 * slots], refs[-1]
        total = jnp.zeros((share, tile), jnp.float32)
        for k in range(slots):
            total += dot(grad_refs[k][...], token_refs[k][...], 0, 0)
        out[...] = total.astype(jnp.bfloat16)

    return pl.pallas_call(
        kernel,
        grid_spec=pltpu.PrefetchScalarGridSpec(
            num_scalar_prefetch=1,
            grid=(width // tile,),
            in_specs=[spec((rows, share), lambda m, side: (0, side[0]))] * slots
            + [spec((rows, tile), lambda m, side: (0, m))] * slots,
            out_specs=spec((share, tile), lambda m, side: (0, m)),
        ),
        out_shape=jax.ShapeDtypeStruct((share, width), jnp.bfloat16),
        cost_estimate=cost(1.1e9, 6e6),
        name="weight_send",
    )(prefetch(core ^ flip), *grads, *tokens)


def weight_pieces(here, core, grads, tokens, received):
    slots = len(grads)
    rows, width = tokens[0].shape
    share = grads[0].shape[1] // 2
    tile = width // slots

    def kernel(*refs):
        grad_refs, token_refs = refs[1 : 1 + slots], refs[1 + slots : 1 + 2 * slots]
        other, outs = refs[1 + 2 * slots], refs[2 + 2 * slots :]
        total = other[...].astype(jnp.float32)
        for k in range(slots):
            total += dot(grad_refs[k][...], token_refs[k][...], 0, 0)
        for k in range(slots):

            @pl.when(pl.program_id(0) == k)
            def _():
                outs[k][...] = total.astype(jnp.bfloat16)

    return pl.pallas_call(
        kernel,
        grid_spec=pltpu.PrefetchScalarGridSpec(
            num_scalar_prefetch=1,
            grid=(slots,),
            in_specs=[spec((rows, share), lambda m, at: (0, at[1]))] * slots
            + [spec((rows, tile), lambda m, at: (0, m ^ at[0]))] * slots
            + [spec((share, tile), lambda m, at: (0, m ^ at[0]))],
            out_specs=[spec((share, tile), lambda m, at: (0, 0))] * slots,
        ),
        out_shape=[jax.ShapeDtypeStruct((share, tile), jnp.bfloat16)] * slots,
        cost_estimate=cost(1.1e9, 6e6),
        name="weight_keep",
    )(prefetch(here, core), *grads, *tokens, received)


def lay_out(here, pieces):
    slots = len(pieces)
    share, tile = pieces[0].shape

    def kernel(*refs):
        out = refs[-1]
        for k in range(slots):

            @pl.when(pl.program_id(0) == k)
            def _():
                out[...] = refs[1 + k][...].astype(jnp.float32)

    return pl.pallas_call(
        kernel,
        grid_spec=pltpu.PrefetchScalarGridSpec(
            num_scalar_prefetch=1,
            grid=(slots,),
            in_specs=[spec((share, tile), lambda m, at: (0, 0))] * slots,
            out_specs=spec((share, tile), lambda m, at: (0, m ^ at[0])),
        ),
        out_shape=jax.ShapeDtypeStruct((share, tile * slots), jnp.float32),
        name="lay_out",
    )(prefetch(here), *pieces)


def gather_slots(array):
    count = lax.axis_size("sp")
    if count != 4:
        return [array] + [swap(array, "sp", k) for k in range(1, count)]
    near, next_ = swap(array, "sp", 1), swap(array, "sp", 2)
    half = array.shape[1] // 2
    far = [swap(next_[:, :half], "sp", 1), swap(near[:, half:], "sp", 2)]
    return [array, near, next_, jnp.concatenate(far, axis=1)]


def direct_body(tokens, key_weight, queries, values, cotangent, log_decay):
    here, member = lax.axis_index("sp"), lax.axis_index("dp")
    slots = lax.axis_size("sp")
    planes = lax.axis_size("dp") // 2
    plane, core = member // 2, member % 2
    seq_len, heads, key_width = queries.shape[1:]
    value_width = values.shape[3]
    rate = lax.dynamic_slice_in_dim(log_decay, here * heads, heads)
    cosine, sine = rotation(seq_len, key_width // 2)
    cosine, sine = cosine[:, 0], sine[:, 0]
    cosine = jnp.concatenate([cosine, cosine], axis=1)
    sine = jnp.concatenate([-sine, sine], axis=1)

    ring = [key_weight]
    for _ in range(planes - 1):
        ring.append(step_planes(ring[-1]))
    shards = [(part, swap(part, "dp", 1)) for part in ring]

    cotans = [columns(cotangent[0], here ^ k, heads * value_width) for k in range(slots)]
    cotans = cotans[:1] + [swap(cotans[k], "sp", k) for k in range(1, slots)]
    token_slots = gather_slots(tokens[0])

    query = queries[0].reshape(seq_len, heads * key_width)
    value = values[0].reshape(seq_len, heads * value_width)
    grads, rotated, mixing, trailing = retention_first(
        here, rate, query, value, cosine, sine, cotans, key_width
    )

    sent = swap(weight_partial(core, grads, token_slots, 1), "dp", 1)
    pieces = list(weight_pieces(here, core, grads, token_slots, sent))
    pieces = pieces[:1] + [swap(pieces[k], "sp", k) for k in range(1, slots)]
    def for_plane(p):
        return lax.select_n((p ^ here).astype(jnp.int32), *pieces) if slots > 2 else lax.select_n(
            (p ^ here) == 1, *pieces
        )

    total = for_plane(plane).astype(jnp.float32)
    for k in range(1, planes):
        total += swap(for_plane(plane ^ k), "dp", 2 * k).astype(jnp.float32)
    grad_weight = lay_out(here, gather_slots(total.astype(jnp.bfloat16)))

    returned = [grads[0]] + [swap(grads[k], "sp", k) for k in range(1, slots)]
    grad_tokens = token_gradient(here, plane, core, returned, shards)

    keys = key_projection(here, plane, core, token_slots, shards)
    grad_query, grad_value = retention_second(
        here, rate, rotated, value, cosine, sine, mixing, trailing, keys, cotans
    )
    return (
        grad_tokens[None],
        grad_query.reshape(queries.shape),
        grad_value.reshape(values.shape),
        grad_weight,
    )


def solution(mesh):
    slots, members = mesh.shape["sp"], mesh.shape["dp"]
    direct = members == 2 * slots and slots & (slots - 1) == 0
    return jax.shard_map(
        direct_body if direct else general_body,
        mesh=mesh,
        in_specs=(
            P("dp", "sp", None),
            P("dp", None),
            P("dp", None, "sp", None),
            P("dp", None, "sp", None),
            P("dp", "sp", None),
            P(),
        ),
        out_specs=(
            P("dp", "sp", None),
            P("dp", None, "sp", None),
            P("dp", None, "sp", None),
            P("dp", None),
        ),
        check_vma=False,
    )
```

```python
import jax
import jax.numpy as jnp
from jax import lax
from jax.experimental import pallas as pl
from jax.experimental.pallas import tpu as pltpu
from jax.sharding import PartitionSpec as P

BLOCK = 128


def product(form, left, right):
    return jnp.einsum(form, left, right, preferred_element_type=jnp.float32)


def rotation(seq_len, half):
    position = jnp.arange(seq_len, dtype=jnp.float32)
    frequency = 10000.0 ** (-jnp.arange(half, dtype=jnp.float32) / half)
    angle = position[:, None] * frequency[None, :]
    return (jnp.cos(angle)[:, None, :], jnp.sin(angle)[:, None, :])


def rotate(vectors, cosine, sine):
    half = vectors.shape[-1] // 2
    front, back = (vectors[..., :half], vectors[..., half:])
    return jnp.concatenate([front * cosine - back * sine, front * sine + back * cosine], axis=-1)


def unrotate(grads, cosine, sine):
    half = grads.shape[-1] // 2
    front, back = (grads[..., :half], grads[..., half:])
    return jnp.concatenate([front * cosine + back * sine, back * cosine - front * sine], axis=-1)


def retention_backward(query_rows, key_rows, value_rows, cotan_rows, head_decay):
    seq_len, heads_here, key_width = query_rows.shape
    nblocks = seq_len // BLOCK
    cosine, sine = rotation(seq_len, key_width // 2)
    factor = key_width ** (-0.5)
    rot_query = rotate(query_rows.astype(jnp.float32), cosine, sine).astype(jnp.bfloat16)
    rot_key = (rotate(key_rows.astype(jnp.float32), cosine, sine) * factor).astype(jnp.bfloat16)

    def blocks(array):
        return array.reshape(nblocks, BLOCK, heads_here, array.shape[-1])

    block_query, block_key = (blocks(rot_query), blocks(rot_key))
    block_value, block_cotan = (blocks(value_rows), blocks(cotan_rows))
    inside = jnp.arange(BLOCK, dtype=jnp.float32)
    offset = inside[:, None] - inside[None, :]
    within = jnp.where(
        offset[None] >= 0, jnp.exp(jnp.maximum(offset, 0.0)[None] * head_decay[:, None, None]), 0.0
    )
    rising = jnp.exp((inside + 1.0)[:, None] * head_decay[None, :])[None, :, :, None]
    falling = jnp.exp((BLOCK - 1.0 - inside)[:, None] * head_decay[None, :])[None, :, :, None]
    scores = (product("nihd,njhd->nhij", block_query, block_key) * within[None]).astype(
        jnp.bfloat16
    )
    mixing = (product("nihe,njhe->nhij", block_cotan, block_value) * within[None]).astype(
        jnp.bfloat16
    )
    decayed_queries = (block_query.astype(jnp.float32) * rising).astype(jnp.bfloat16)
    decayed_keys = (block_key.astype(jnp.float32) * falling).astype(jnp.bfloat16)
    block_states = product("nihd,nihe->nhde", decayed_keys, block_value)
    block_trails = product("nihd,nihe->nhde", decayed_queries, block_cotan)
    block_index = jnp.arange(nblocks, dtype=jnp.float32)
    spacing = block_index[:, None] - block_index[None, :] - 1.0
    earlier = jnp.where(
        spacing[None] >= 0,
        jnp.exp(jnp.maximum(spacing, 0.0)[None] * BLOCK * head_decay[:, None, None]),
        0.0,
    )
    later = jnp.transpose(earlier, (0, 2, 1))
    entering = jnp.einsum(
        "hnm,mhde->nhde", earlier, block_states, precision=lax.Precision.HIGHEST
    ).astype(jnp.bfloat16)
    trailing = jnp.einsum(
        "hnm,mhde->nhde", later, block_trails, precision=lax.Precision.HIGHEST
    ).astype(jnp.bfloat16)
    grad_rq = product("nhij,njhd->nihd", mixing, block_key) + rising * product(
        "nihe,nhde->nihd", block_cotan, entering
    )
    grad_rk = product("nhij,nihd->njhd", mixing, block_query) + falling * product(
        "nihe,nhde->nihd", block_value, trailing
    )
    grad_value = product("nhij,nihe->njhe", scores, block_cotan) + falling * product(
        "nihd,nhde->nihe", block_key, trailing
    )
    grad_rq = grad_rq.reshape(seq_len, heads_here, key_width)
    grad_rk = grad_rk.reshape(seq_len, heads_here, key_width)
    grad_query = unrotate(grad_rq, cosine, sine).astype(jnp.bfloat16)
    grad_key = (unrotate(grad_rk, cosine, sine) * factor).astype(jnp.bfloat16)
    grad_value = grad_value.reshape(seq_len, heads_here, -1).astype(jnp.bfloat16)
    return (grad_query, grad_key, grad_value)


def general_body(tokens, key_weight, queries, values, cotangent, log_decay):
    gathered = lax.all_gather(key_weight, "dp", axis=0, tiled=True)
    token_rows = tokens[0]
    key_proj = jnp.einsum(
        "td,qd->tq", token_rows, gathered, preferred_element_type=jnp.float32
    ).astype(jnp.bfloat16)
    head_keys, head_cotan = (
        lax.all_to_all(key_proj[None], "sp", split_axis=2, concat_axis=1, tiled=True),
        lax.all_to_all(cotangent, "sp", split_axis=2, concat_axis=1, tiled=True),
    )
    seq_len = head_keys.shape[1]
    heads_here = queries.shape[2]
    head_start = lax.axis_index("sp") * heads_here
    head_decay = lax.dynamic_slice_in_dim(log_decay, head_start, heads_here)
    grad_query, grad_key, grad_value = retention_backward(
        queries[0],
        head_keys[0].reshape(seq_len, heads_here, -1),
        values[0],
        head_cotan[0].reshape(seq_len, heads_here, -1),
        head_decay,
    )
    returned = lax.all_to_all(
        grad_key.reshape(1, seq_len, -1), "sp", split_axis=1, concat_axis=2, tiled=True
    )
    key_grads = returned[0]
    grad_tokens = jnp.dot(key_grads, gathered, preferred_element_type=jnp.float32).astype(
        jnp.bfloat16
    )
    width = key_grads.shape[1]
    count_dp = lax.axis_size("dp")
    count_sp = lax.axis_size("sp")
    share = width // (count_sp * count_dp)
    ordered = (
        key_grads.reshape(-1, count_dp, count_sp, share).transpose(0, 2, 1, 3).reshape(-1, width)
    )
    partial_grad = jnp.einsum("tq,td->qd", ordered, token_rows, preferred_element_type=jnp.float32)
    owned = lax.psum_scatter(partial_grad, ("sp", "dp"), scatter_dimension=0, tiled=True)
    weight_grad = lax.all_gather(owned, "sp", axis=0, tiled=True)
    return (grad_tokens[None], grad_query[None], grad_value[None], weight_grad)


INNER = 256
CHUNKS = 1


def swap(array, axis, bit):
    count = lax.axis_size(axis)
    return lax.ppermute(array, axis, [(i, i ^ bit) for i in range(count)])


def step_planes(array):
    count = lax.axis_size("dp")
    return lax.ppermute(array, "dp", [(i, (i + 2) % count) for i in range(count)])


def limit(mib):
    return pltpu.CompilerParams(vmem_limit_bytes=mib * 2**20)


def dot(left, right, left_dim, right_dim):
    return lax.dot_general(
        left, right, (((left_dim,), (right_dim,)), ((), ())), preferred_element_type=jnp.float32
    )


def columns(array, index, width):
    return lax.dynamic_slice_in_dim(array, index * width, width, axis=1)


def cost(flops, moved):
    return pl.CostEstimate(flops=int(flops), bytes_accessed=int(moved), transcendentals=0)


def spec(shape, index):
    return pl.BlockSpec(shape, index)


def decays(rate, size):
    rows = lax.broadcasted_iota(jnp.int32, (size, size), 0)
    cols = lax.broadcasted_iota(jnp.int32, (size, size), 1)
    gap = (rows - cols).astype(jnp.float32)
    within = jnp.where(gap >= 0, jnp.exp(jnp.maximum(gap, 0.0) * rate), 0.0)
    flipped = jnp.where(gap <= 0, jnp.exp(jnp.maximum(-gap, 0.0) * rate), 0.0)
    place = lax.broadcasted_iota(jnp.int32, (size, 1), 0).astype(jnp.float32)
    rising = jnp.exp((place + 1.0) * rate)
    falling = jnp.exp((size - 1.0 - place) * rate)
    whole = jnp.exp(jnp.full((1, 1), float(size), jnp.float32) * rate)
    return within, flipped, rising, falling, whole


def turn(block, cosine, sine):
    half = block.shape[-1] // 2
    return block * cosine + pltpu.roll(block, half, 1) * sine


def turn_back(block, cosine, sine):
    half = block.shape[-1] // 2
    return block * cosine - pltpu.roll(block, half, 1) * sine


def first_kernel(slots, rows, inner, factor):
    def kernel(*refs):
        place, rate_ref, query, value, cosine, sine = refs[:6]
        cotans = refs[6 : 6 + slots]
        outs = refs[6 + slots :]
        grads, turned_grads = outs[:slots], outs[slots : 2 * slots]
        rotated, trailing, cotan, whole_grad, flat_grad = outs[2 * slots :]
        here = place[0]
        rate = rate_ref[pl.program_id(0)]
        for k in range(slots):
            cotan[pl.ds((here ^ k) * rows, rows), :] = cotans[k][...]
        _, flipped, rising, falling, whole = decays(rate, inner)
        seq_len = query.shape[0]
        carry = jnp.zeros((query.shape[1], value.shape[1]), jnp.float32)
        for n in reversed(range(seq_len // inner)):
            at = slice(n * inner, (n + 1) * inner)
            cos, sin = cosine[at, :], sine[at, :]
            turned = turn(query[at, :].astype(jnp.float32), cos, sin).astype(jnp.bfloat16)
            rotated[at, :] = turned
            co, va = cotan[at, :], value[at, :]
            mix = (dot(va, co, 1, 1) * flipped).astype(jnp.bfloat16)
            trail = carry.astype(jnp.bfloat16)
            trailing[0, n] = trail
            grad = dot(mix, turned, 1, 0) + falling * dot(va, trail, 1, 1)
            grad = turn_back(grad, cos, sin) * factor
            whole_grad[at, :] = grad.astype(jnp.bfloat16)
            start = n * inner % rows
            flat_grad[n * inner // rows, :, start : start + inner] = grad.T.astype(jnp.bfloat16)
            decayed = (turned.astype(jnp.float32) * rising).astype(jnp.bfloat16)
            carry = carry * whole + dot(decayed, co, 0, 0)
        for k in range(slots):
            grads[k][...] = whole_grad[pl.ds((here ^ k) * rows, rows), :]
            turned_grads[k][...] = flat_grad[here ^ k]

    return kernel


def second_kernel(slots, rows, inner, factor):
    def kernel(*refs):
        place, rate_ref, rotated, value, cosine, sine, trailing, keys = refs[:8]
        cotans = refs[8 : 8 + slots]
        grad_query, grad_value, cotan, key = refs[8 + slots :]
        here = place[0]
        rate = rate_ref[pl.program_id(0)]
        for k in range(slots):
            at = pl.ds((here ^ k) * rows, rows)
            cotan[at, :] = cotans[k][...]
            key[at, :] = keys[k * rows : (k + 1) * rows, :]
        within, flipped, rising, falling, whole = decays(rate, inner)
        seq_len = rotated.shape[0]
        carry = jnp.zeros((rotated.shape[1], value.shape[1]), jnp.float32)
        for n in range(seq_len // inner):
            at = slice(n * inner, (n + 1) * inner)
            cos, sin = cosine[at, :], sine[at, :]
            rk = (turn(key[at, :].astype(jnp.float32), cos, sin) * factor).astype(jnp.bfloat16)
            rq, co, va = rotated[at, :], cotan[at, :], value[at, :]
            score = (dot(rk, rq, 1, 1) * flipped).astype(jnp.bfloat16)
            entering = carry.astype(jnp.bfloat16)
            mix = (dot(co, va, 1, 1) * within).astype(jnp.bfloat16)
            grad = dot(mix, rk, 1, 0) + rising * dot(co, entering, 1, 1)
            grad_query[at, :] = turn_back(grad, cos, sin).astype(jnp.bfloat16)
            grad_value[at, :] = (
                dot(score, co, 1, 0) + falling * dot(rk, trailing[0, n], 1, 0)
            ).astype(jnp.bfloat16)
            decayed = (rk.astype(jnp.float32) * falling).astype(jnp.bfloat16)
            carry = carry * whole + dot(decayed, va, 0, 0)

    return kernel


def prefetch(*values):
    return jnp.stack([jnp.asarray(v, jnp.int32) for v in values])


def near(count=1):
    return [pl.BlockSpec(memory_space=pltpu.VMEM)] * count


def away(count=1):
    return [pl.BlockSpec(memory_space=pltpu.HBM)] * count


def smem():
    return pl.BlockSpec(memory_space=pltpu.SMEM)


def retention_first(here, rate, query, value, cosine, sine, cotans, key_width):
    slots = len(cotans)
    seq_len, query_width = query.shape
    heads = query_width // key_width
    value_width = value.shape[1] // heads
    rows = cotans[0].shape[0]
    inner = min(INNER, rows)
    nblocks = seq_len // inner
    half = jnp.bfloat16
    full = spec((seq_len, key_width), lambda h: (0, 0))
    head = spec((seq_len, key_width), lambda h: (0, h))
    outs = [pltpu.HBM((rows, query_width), half)] * slots
    outs += [pltpu.HBM((query_width, rows), half)] * slots
    outs += [
        pltpu.HBM((seq_len, query_width), half),
        pltpu.HBM((heads, nblocks, key_width, value_width), half),
    ]
    result = pl.pallas_call(
        first_kernel(slots, rows, inner, key_width**-0.5),
        grid=(heads,),
        in_specs=[smem(), smem(), head, spec((seq_len, value_width), lambda h: (0, h)), full, full]
        + [spec((rows, value_width), lambda h: (0, h))] * slots,
        out_specs=[spec((rows, key_width), lambda h: (0, h))] * slots
        + [spec((key_width, rows), lambda h: (h, 0))] * slots
        + [
            head,
            spec((1, nblocks, key_width, value_width), lambda h: (h, 0, 0, 0)),
        ],
        out_shape=outs,
        scratch_shapes=[
            pltpu.VMEM((seq_len, value_width), half),
            pltpu.VMEM((seq_len, key_width), half),
            pltpu.VMEM((slots, key_width, rows), half),
        ],
        compiler_params=limit(16),
        cost_estimate=cost(6e9, 10e6),
        name="retention_first",
    )(prefetch(here), rate, query, value, cosine, sine, *cotans)
    return list(result[:slots]), list(result[slots : 2 * slots]), *result[2 * slots :]


def retention_second(here, rate, rotated, value, cosine, sine, trailing, keys, cotans):
    slots = len(cotans)
    heads, nblocks, key_width, value_width = trailing.shape
    seq_len = rotated.shape[0]
    inner = seq_len // nblocks
    rows = cotans[0].shape[0]
    half = jnp.bfloat16
    full = spec((seq_len, key_width), lambda h: (0, 0))
    head = spec((seq_len, key_width), lambda h: (0, h))
    wide = spec((seq_len, value_width), lambda h: (0, h))
    return pl.pallas_call(
        second_kernel(slots, rows, inner, key_width**-0.5),
        grid=(heads,),
        in_specs=[
            smem(),
            smem(),
            head,
            wide,
            full,
            full,
            spec((1, nblocks, key_width, value_width), lambda h: (h, 0, 0, 0)),
            spec((slots * rows, key_width), lambda h: (0, h)),
        ]
        + [spec((rows, value_width), lambda h: (0, h))] * slots,
        out_specs=[head, wide],
        out_shape=[
            pltpu.HBM(rotated.shape, half),
            pltpu.HBM(value.shape, half),
        ],
        scratch_shapes=[
            pltpu.VMEM((seq_len, value_width), half),
            pltpu.VMEM((seq_len, key_width), half),
        ],
        compiler_params=limit(16),
        cost_estimate=cost(6e9, 14e6),
        name="retention_second",
    )(prefetch(here), rate, rotated, value, cosine, sine, trailing, keys, *cotans)


def halves(tokens):
    width = sum(part.shape[1] for part in tokens[0])
    found, place = ([], []), 0
    for k, parts in enumerate(tokens):
        for at, part in place_parts(parts):
            for piece in range(2 * part.shape[1] // width):
                found[2 * at // width + piece].append((k, place, piece))
            place += 1
    return found


def key_projection(here, plane, core, tokens, shards):
    slots = len(tokens)
    planes = len(shards)
    parts = [part for slot in tokens for part in slot]
    loads = halves(tokens)
    rows, width = tokens[0][0].shape[0], sum(part.shape[1] for part in tokens[0])
    share = shards[0][0].shape[0]
    half = width // 2

    def kernel(*refs):
        place = refs[0]
        token_refs = refs[1 : 1 + len(parts)]
        shard_refs = refs[1 + len(parts) : 1 + len(parts) + 2 * planes]
        out, weight, token, total, sems = refs[1 + len(parts) + 2 * planes :]
        slot, own = place[0], place[1]

        def weight_copy(r, side, at):
            return pltpu.make_async_copy(
                shard_refs[2 * r + side].at[:, at * half : (at + 1) * half],
                weight.at[at, pl.ds(pl.multiple_of((own ^ side) * share, share), share)],
                sems.at[at, slots + side],
            )

        def token_copy(at, k, index, piece):
            return pltpu.make_async_copy(
                token_refs[index].at[:, piece * half : (piece + 1) * half],
                token.at[at, k * rows : (k + 1) * rows],
                sems.at[at, k],
            )

        for at in range(2):
            for r in range(planes):

                @pl.when(slot == r)
                def _():
                    for side in range(2):
                        weight_copy(r, side, at).start()

            for k, index, piece in loads[at]:
                token_copy(at, k, index, piece).start()
        for at in range(2):
            for side in range(2):
                weight_copy(0, side, at).wait()
            for k, index, piece in loads[at]:
                token_copy(at, k, index, piece).wait()
            term = dot(token[at], weight[at], 1, 1)
            if at == 0:
                total[...] = term
            else:
                out[...] = (total[...] + term).astype(jnp.bfloat16)

    far = len(tokens[-1])
    return pl.pallas_call(
        kernel,
        in_specs=[smem()] + away(len(parts) - far) + near(far) + away(2 * planes),
        out_specs=near()[0],
        out_shape=pltpu.VMEM((slots * rows, 2 * share), jnp.bfloat16),
        scratch_shapes=[
            pltpu.VMEM((2, 2 * share, half), jnp.bfloat16),
            pltpu.VMEM((2, slots * rows, half), jnp.bfloat16),
            pltpu.VMEM((slots * rows, 2 * share), jnp.float32),
            pltpu.SemaphoreType.DMA((2, slots + 2)),
        ],
        compiler_params=limit(20),
        cost_estimate=cost(4e9, 8e6),
        name="key_projection",
    )(
        prefetch((plane - here) % planes, core),
        *parts,
        *[part for pair in shards for part in pair],
    )


def token_gradient(here, plane, core, grads, shards):
    slots = len(grads)
    planes = len(shards)
    rows = grads[0].shape[0]
    share, width = shards[0][0].shape

    def kernel(*refs):
        place = refs[0]
        grad_refs = refs[1 : 1 + slots]
        shard_refs = refs[1 + slots : 1 + slots + 2 * planes]
        out, grad, weight, total, sems = refs[1 + slots + 2 * planes :]
        own = place[2]

        def grad_copy(k):
            return pltpu.make_async_copy(grad_refs[k], grad.at[k], sems.at[2 * planes + k])

        def shard_copy(r, side):
            return pltpu.make_async_copy(
                shard_refs[2 * r + side], weight.at[r, own ^ side], sems.at[2 * r + side]
            )

        for k in range(slots):
            grad_copy(k).start()
        for r in range(planes):
            for side in range(2):
                shard_copy(r, side).start()
        for k in range(slots):
            grad_copy(k).wait()
        for r in range(planes):
            k = ((place[1] + planes - r) % planes) ^ place[0]
            for side in range(2):
                shard_copy(r, side).wait()
            block = grad[k]
            term = dot(block[:, :share], weight[r, 0], 1, 0)
            term += dot(block[:, share:], weight[r, 1], 1, 0)
            if r == 0:
                total[...] = term
            elif r < planes - 1:
                total[...] += term
            else:
                out[...] = (total[...] + term).astype(jnp.bfloat16)

    return pl.pallas_call(
        kernel,
        in_specs=[smem()] + away(slots + 2 * planes),
        out_specs=near()[0],
        out_shape=jax.ShapeDtypeStruct((rows, width), jnp.bfloat16),
        scratch_shapes=[
            pltpu.VMEM((slots, rows, 2 * share), jnp.bfloat16),
            pltpu.VMEM((planes, 2, share, width), jnp.bfloat16),
            pltpu.VMEM((rows, width), jnp.float32),
            pltpu.SemaphoreType.DMA((2 * planes + slots,)),
        ],
        compiler_params=limit(20),
        cost_estimate=cost(5e9, 11e6),
        name="token_gradient",
    )(prefetch(here, plane, core), *grads, *[part for pair in shards for part in pair])


def place_parts(parts):
    at, placed = 0, []
    for part in parts:
        placed.append((at, part))
        at += part.shape[1]
    return placed


def weight_start(grads, tokens):
    slots = len(tokens)
    features, rows = grads[0].shape
    parts = [part for slot in tokens for part in slot]
    loads = halves(tokens)
    width = sum(part.shape[1] for part in tokens[0])
    half = width // 2

    def kernel(*refs):
        grad_refs, token_refs = refs[: slots + 1], refs[slots + 1 : slots + 1 + len(parts)]
        out, last, grad, token, sems, grad_sems = refs[slots + 1 + len(parts) :]

        def fetch(at, k, index, piece):
            return pltpu.make_async_copy(
                token_refs[index].at[:, piece * half : (piece + 1) * half],
                token.at[at, k],
                sems.at[at, k],
            )

        def fetch_grad(k):
            to = grad.at[k] if k < slots else last
            return pltpu.make_async_copy(grad_refs[k], to, grad_sems.at[k])

        for k in range(slots):
            fetch_grad(k).start()
        for at in range(2):
            for load in loads[at]:
                fetch(at, *load).start()
        fetch_grad(slots).start()
        for k in range(slots):
            fetch_grad(k).wait()
        for at in range(2):
            for load in loads[at]:
                fetch(at, *load).wait()
            total = dot(grad[0], token[at, 0], 1, 0)
            for k in range(1, slots):
                total += dot(grad[k], token[at, k], 1, 0)
            out[:, at * half : (at + 1) * half] = total
        fetch_grad(slots).wait()

    return pl.pallas_call(
        kernel,
        in_specs=away(slots + 1 + len(parts)),
        out_specs=near(2),
        out_shape=[
            pltpu.VMEM((features, width), jnp.float32),
            pltpu.VMEM((features, rows), jnp.bfloat16),
        ],
        scratch_shapes=[
            pltpu.VMEM((slots, features, rows), jnp.bfloat16),
            pltpu.VMEM((2, slots, rows, half), jnp.bfloat16),
            pltpu.SemaphoreType.DMA((2, slots)),
            pltpu.SemaphoreType.DMA((slots + 1,)),
        ],
        compiler_params=limit(20),
        cost_estimate=cost(4e9, 6e6),
        name="weight_start",
    )(*grads, *parts)


def weight_end(core, grad, tokens, total):
    features, width = total.shape
    share = features // 2

    def kernel(place, grad_ref, *refs):
        token_refs, (so_far, sent, kept) = refs[: len(tokens)], refs[len(tokens) :]
        own = place[0]
        for (at, part), ref in zip(place_parts(tokens), token_refs):
            to = slice(at, at + part.shape[1])
            rows = pl.ds(pl.multiple_of((own ^ 1) * share, share), share)
            sent[:, to] = (so_far[rows, to] + dot(grad_ref[rows, :], ref[...], 1, 0)).astype(
                jnp.bfloat16
            )
        for (at, part), ref in zip(place_parts(tokens), token_refs):
            to = slice(at, at + part.shape[1])
            rows = pl.ds(pl.multiple_of(own * share, share), share)
            kept[:, to] = so_far[rows, to] + dot(grad_ref[rows, :], ref[...], 1, 0)

    return pl.pallas_call(
        kernel,
        in_specs=[smem()] + near(2 + len(tokens)),
        out_specs=near(2),
        out_shape=[
            pltpu.VMEM((share, width), jnp.bfloat16),
            pltpu.VMEM((share, width), jnp.float32),
        ],
        compiler_params=limit(20),
        cost_estimate=cost(4e9, 6e6),
        name="weight_end",
    )(prefetch(core), grad, *tokens, total)


def weight_pieces(here, slots, kept, received):
    share, width = kept.shape
    tile = width // slots

    def kernel(place, own, other, *outs):
        for k in range(slots):
            at = pl.ds(pl.multiple_of((place[0] ^ k) * tile, tile), tile)
            outs[k][...] = (own[:, at] + other[:, at].astype(jnp.float32)).astype(jnp.bfloat16)

    return pl.pallas_call(
        kernel,
        in_specs=[smem()] + near(2),
        out_specs=near(slots),
        out_shape=[pltpu.VMEM((share, tile), jnp.bfloat16)] * slots,
        compiler_params=limit(12),
        cost_estimate=cost(2e9, 6e6),
        name="weight_pieces",
    )(prefetch(here), kept, received)


def route(here, plane, planes, chunks, pieces):
    slots = len(pieces)
    share, tile = pieces[0].shape
    size = tile // chunks

    def kernel(place, *refs):
        outs, stack = refs[slots:-1], refs[-1]
        for k in range(slots):
            stack[k] = refs[k][...]
        for k in range(planes):
            slot = place[0] ^ place[1] ^ k
            for chunk in range(chunks):
                outs[chunk * planes + k][...] = stack[slot, :, chunk * size : (chunk + 1) * size]

    result = pl.pallas_call(
        kernel,
        in_specs=[smem()] + near(slots),
        out_specs=near(planes * chunks),
        out_shape=[pltpu.VMEM((share, size), jnp.bfloat16)] * (planes * chunks),
        scratch_shapes=[pltpu.VMEM((slots, share, tile), jnp.bfloat16)],
        compiler_params=limit(12),
        cost_estimate=cost(1e9, 2e6),
        name="route",
    )(prefetch(here, plane), *pieces)
    return [result[chunk * planes : (chunk + 1) * planes] for chunk in range(chunks)]


def add_up(terms):
    def kernel(*refs):
        total = refs[0][...].astype(jnp.float32)
        for ref in refs[1:-1]:
            total += ref[...].astype(jnp.float32)
        refs[-1][...] = total.astype(jnp.bfloat16)

    return pl.pallas_call(
        kernel,
        in_specs=near(len(terms)),
        out_specs=near()[0],
        out_shape=pltpu.VMEM(terms[0].shape, jnp.bfloat16),
        compiler_params=limit(12),
        cost_estimate=cost(1e9, 1e6),
        name="add_up",
    )(*terms)


def lay_out(here, pieces, chunk, chunks, out=None):
    slots = len(pieces)
    share, size = pieces[0].shape
    shape = jax.ShapeDtypeStruct((share, size * chunks * slots), jnp.float32)
    given = [] if out is None else [out]

    def kernel(place, *refs):
        target, wide, sems = refs[slots + len(given) :]

        def store(k):
            at = ((place[0] ^ k) * chunks + chunk) * size
            return pltpu.make_async_copy(
                wide.at[k], target.at[:, pl.ds(pl.multiple_of(at, size), size)], sems.at[k]
            )

        for k in range(slots):
            wide[k] = refs[k][...].astype(jnp.float32)
            store(k).start()
        for k in range(slots):
            store(k).wait()

    return pl.pallas_call(
        kernel,
        in_specs=[smem()] + near(slots) + away(len(given)),
        out_specs=away()[0],
        out_shape=shape,
        input_output_aliases={1 + slots: 0} if given else {},
        scratch_shapes=[
            pltpu.VMEM((slots, share, size), jnp.float32),
            pltpu.SemaphoreType.DMA((slots,)),
        ],
        compiler_params=limit(12),
        cost_estimate=cost(1e9, 4e6),
        name="lay_out",
    )(prefetch(here), *pieces, *given)


def gather_slots(array):
    half = array.shape[1] // 2
    low, high = array[:, :half], array[:, half:]
    near_high, next_low = swap(high, "sp", 1), swap(low, "sp", 2)
    near_low, next_high = swap(low, "sp", 1), swap(high, "sp", 2)
    far = [swap(next_low, "sp", 1), swap(near_high, "sp", 2)]
    return [[array], [near_low, near_high], [next_low, next_high], far]


def direct_body(tokens, key_weight, queries, values, cotangent, log_decay):
    return direct_steps(tokens, key_weight, queries, values, cotangent, log_decay)


def direct_steps(tokens, key_weight, queries, values, cotangent, log_decay):
    here, member = lax.axis_index("sp"), lax.axis_index("dp")
    slots = lax.axis_size("sp")
    planes = lax.axis_size("dp") // 2
    plane, core = member // 2, member % 2
    seq_len, heads, key_width = queries.shape[1:]
    value_width = values.shape[3]
    rate = lax.dynamic_slice_in_dim(log_decay, here * heads, heads)
    cosine, sine = rotation(seq_len, key_width // 2)
    cosine, sine = cosine[:, 0], sine[:, 0]
    cosine = jnp.concatenate([cosine, cosine], axis=1)
    sine = jnp.concatenate([-sine, sine], axis=1)

    ring = [key_weight]
    for _ in range(1, planes):
        ring.append(step_planes(ring[-1]))
    shards = [(part, swap(part, "dp", 1)) for part in ring]

    cotans = [columns(cotangent[0], here ^ k, heads * value_width) for k in range(slots)]
    cotans = cotans[:1] + [swap(cotans[k], "sp", k) for k in range(1, slots)]
    token_slots = gather_slots(tokens[0])

    query = queries[0].reshape(seq_len, heads * key_width)
    value = values[0].reshape(seq_len, heads * value_width)
    grads, turned_grads, rotated, trailing = retention_first(
        here, rate, query, value, cosine, sine, cotans, key_width
    )

    total, last = weight_start(turned_grads, token_slots[:-1])
    sent, kept = weight_end(core, last, token_slots[-1], total)
    received = swap(sent, "dp", 1)
    pieces = list(weight_pieces(here, slots, kept, received))
    pieces = pieces[:1] + [swap(pieces[k], "sp", k) for k in range(1, slots)]

    routed = route(here, plane, planes, CHUNKS, pieces)
    grad_weight = None
    for chunk, arrays in enumerate(routed):
        terms = [arrays[0]]
        terms += [swap(arrays[k], "dp", 2 * k) for k in range(1, planes)]
        total = add_up(terms)
        gathered = [total] + [swap(total, "sp", k) for k in range(1, slots)]
        grad_weight = lay_out(here, gathered, chunk, CHUNKS, grad_weight)

    returned = [grads[0]] + [swap(grads[k], "sp", k) for k in range(1, slots)]
    grad_tokens = token_gradient(here, plane, core, returned, shards)

    keys = key_projection(here, plane, core, token_slots, shards)
    grad_query, grad_value = retention_second(
        here, rate, rotated, value, cosine, sine, trailing, keys, cotans
    )
    grad_query = grad_query.reshape(queries.shape)
    grad_value = grad_value.reshape(values.shape)
    return (
        grad_tokens[None],
        grad_query,
        grad_value,
        grad_weight,
    )


def solution(mesh):
    slots, members = mesh.shape["sp"], mesh.shape["dp"]
    direct = members == 2 * slots and slots == 4
    return jax.shard_map(
        direct_body if direct else general_body,
        mesh=mesh,
        in_specs=(
            P("dp", "sp", None),
            P("dp", None),
            P("dp", None, "sp", None),
            P("dp", None, "sp", None),
            P("dp", "sp", None),
            P(),
        ),
        out_specs=(
            P("dp", "sp", None),
            P("dp", None, "sp", None),
            P("dp", None, "sp", None),
            P("dp", None),
        ),
        check_vma=False,
    )
```

```python
import jax
import jax.numpy as jnp
from jax import lax
from jax.experimental import pallas as pl
from jax.experimental.pallas import tpu as pltpu
from jax.sharding import PartitionSpec as P

BLOCK = 128


def product(form, left, right):
    return jnp.einsum(form, left, right, preferred_element_type=jnp.float32)


def rotation(seq_len, half):
    position = jnp.arange(seq_len, dtype=jnp.float32)
    frequency = 10000.0 ** (-jnp.arange(half, dtype=jnp.float32) / half)
    angle = position[:, None] * frequency[None, :]
    return (jnp.cos(angle)[:, None, :], jnp.sin(angle)[:, None, :])


def rotate(vectors, cosine, sine):
    half = vectors.shape[-1] // 2
    front, back = (vectors[..., :half], vectors[..., half:])
    return jnp.concatenate([front * cosine - back * sine, front * sine + back * cosine], axis=-1)


def unrotate(grads, cosine, sine):
    half = grads.shape[-1] // 2
    front, back = (grads[..., :half], grads[..., half:])
    return jnp.concatenate([front * cosine + back * sine, back * cosine - front * sine], axis=-1)


def retention_backward(query_rows, key_rows, value_rows, cotan_rows, head_decay):
    seq_len, heads_here, key_width = query_rows.shape
    nblocks = seq_len // BLOCK
    cosine, sine = rotation(seq_len, key_width // 2)
    factor = key_width ** (-0.5)
    rot_query = rotate(query_rows.astype(jnp.float32), cosine, sine).astype(jnp.bfloat16)
    rot_key = (rotate(key_rows.astype(jnp.float32), cosine, sine) * factor).astype(jnp.bfloat16)

    def blocks(array):
        return array.reshape(nblocks, BLOCK, heads_here, array.shape[-1])

    block_query, block_key = (blocks(rot_query), blocks(rot_key))
    block_value, block_cotan = (blocks(value_rows), blocks(cotan_rows))
    inside = jnp.arange(BLOCK, dtype=jnp.float32)
    offset = inside[:, None] - inside[None, :]
    within = jnp.where(
        offset[None] >= 0, jnp.exp(jnp.maximum(offset, 0.0)[None] * head_decay[:, None, None]), 0.0
    )
    rising = jnp.exp((inside + 1.0)[:, None] * head_decay[None, :])[None, :, :, None]
    falling = jnp.exp((BLOCK - 1.0 - inside)[:, None] * head_decay[None, :])[None, :, :, None]
    scores = (product("nihd,njhd->nhij", block_query, block_key) * within[None]).astype(
        jnp.bfloat16
    )
    mixing = (product("nihe,njhe->nhij", block_cotan, block_value) * within[None]).astype(
        jnp.bfloat16
    )
    decayed_queries = (block_query.astype(jnp.float32) * rising).astype(jnp.bfloat16)
    decayed_keys = (block_key.astype(jnp.float32) * falling).astype(jnp.bfloat16)
    block_states = product("nihd,nihe->nhde", decayed_keys, block_value)
    block_trails = product("nihd,nihe->nhde", decayed_queries, block_cotan)
    block_index = jnp.arange(nblocks, dtype=jnp.float32)
    spacing = block_index[:, None] - block_index[None, :] - 1.0
    earlier = jnp.where(
        spacing[None] >= 0,
        jnp.exp(jnp.maximum(spacing, 0.0)[None] * BLOCK * head_decay[:, None, None]),
        0.0,
    )
    later = jnp.transpose(earlier, (0, 2, 1))
    entering = jnp.einsum(
        "hnm,mhde->nhde", earlier, block_states, precision=lax.Precision.HIGHEST
    ).astype(jnp.bfloat16)
    trailing = jnp.einsum(
        "hnm,mhde->nhde", later, block_trails, precision=lax.Precision.HIGHEST
    ).astype(jnp.bfloat16)
    grad_rq = product("nhij,njhd->nihd", mixing, block_key) + rising * product(
        "nihe,nhde->nihd", block_cotan, entering
    )
    grad_rk = product("nhij,nihd->njhd", mixing, block_query) + falling * product(
        "nihe,nhde->nihd", block_value, trailing
    )
    grad_value = product("nhij,nihe->njhe", scores, block_cotan) + falling * product(
        "nihd,nhde->nihe", block_key, trailing
    )
    grad_rq = grad_rq.reshape(seq_len, heads_here, key_width)
    grad_rk = grad_rk.reshape(seq_len, heads_here, key_width)
    grad_query = unrotate(grad_rq, cosine, sine).astype(jnp.bfloat16)
    grad_key = (unrotate(grad_rk, cosine, sine) * factor).astype(jnp.bfloat16)
    grad_value = grad_value.reshape(seq_len, heads_here, -1).astype(jnp.bfloat16)
    return (grad_query, grad_key, grad_value)


def general_body(tokens, key_weight, queries, values, cotangent, log_decay):
    gathered = lax.all_gather(key_weight, "dp", axis=0, tiled=True)
    token_rows = tokens[0]
    key_proj = jnp.einsum(
        "td,qd->tq", token_rows, gathered, preferred_element_type=jnp.float32
    ).astype(jnp.bfloat16)
    head_keys, head_cotan = (
        lax.all_to_all(key_proj[None], "sp", split_axis=2, concat_axis=1, tiled=True),
        lax.all_to_all(cotangent, "sp", split_axis=2, concat_axis=1, tiled=True),
    )
    seq_len = head_keys.shape[1]
    heads_here = queries.shape[2]
    head_start = lax.axis_index("sp") * heads_here
    head_decay = lax.dynamic_slice_in_dim(log_decay, head_start, heads_here)
    grad_query, grad_key, grad_value = retention_backward(
        queries[0],
        head_keys[0].reshape(seq_len, heads_here, -1),
        values[0],
        head_cotan[0].reshape(seq_len, heads_here, -1),
        head_decay,
    )
    returned = lax.all_to_all(
        grad_key.reshape(1, seq_len, -1), "sp", split_axis=1, concat_axis=2, tiled=True
    )
    key_grads = returned[0]
    grad_tokens = jnp.dot(key_grads, gathered, preferred_element_type=jnp.float32).astype(
        jnp.bfloat16
    )
    width = key_grads.shape[1]
    count_dp = lax.axis_size("dp")
    count_sp = lax.axis_size("sp")
    share = width // (count_sp * count_dp)
    ordered = (
        key_grads.reshape(-1, count_dp, count_sp, share).transpose(0, 2, 1, 3).reshape(-1, width)
    )
    partial_grad = jnp.einsum("tq,td->qd", ordered, token_rows, preferred_element_type=jnp.float32)
    owned = lax.psum_scatter(partial_grad, ("sp", "dp"), scatter_dimension=0, tiled=True)
    weight_grad = lax.all_gather(owned, "sp", axis=0, tiled=True)
    return (grad_tokens[None], grad_query[None], grad_value[None], weight_grad)


INNER = 256
CHUNKS = 2


def swap(array, axis, bit):
    count = lax.axis_size(axis)
    return lax.ppermute(array, axis, [(i, i ^ bit) for i in range(count)])


def step_planes(array):
    count = lax.axis_size("dp")
    return lax.ppermute(array, "dp", [(i, (i + 2) % count) for i in range(count)])


def limit(mib):
    return pltpu.CompilerParams(vmem_limit_bytes=mib * 2**20)


def dot(left, right, left_dim, right_dim):
    return lax.dot_general(
        left, right, (((left_dim,), (right_dim,)), ((), ())), preferred_element_type=jnp.float32
    )


def columns(array, index, width):
    return lax.dynamic_slice_in_dim(array, index * width, width, axis=1)


def cost(flops, moved):
    return pl.CostEstimate(flops=int(flops), bytes_accessed=int(moved), transcendentals=0)


def spec(shape, index):
    return pl.BlockSpec(shape, index)


def decays(rate, size):
    rows = lax.broadcasted_iota(jnp.int32, (size, size), 0)
    cols = lax.broadcasted_iota(jnp.int32, (size, size), 1)
    gap = (rows - cols).astype(jnp.float32)
    within = jnp.where(gap >= 0, jnp.exp(jnp.maximum(gap, 0.0) * rate), 0.0)
    flipped = jnp.where(gap <= 0, jnp.exp(jnp.maximum(-gap, 0.0) * rate), 0.0)
    place = lax.broadcasted_iota(jnp.int32, (size, 1), 0).astype(jnp.float32)
    rising = jnp.exp((place + 1.0) * rate)
    falling = jnp.exp((size - 1.0 - place) * rate)
    whole = jnp.exp(jnp.full((1, 1), float(size), jnp.float32) * rate)
    return within, flipped, rising, falling, whole


def turn(block, cosine, sine):
    half = block.shape[-1] // 2
    return block * cosine + pltpu.roll(block, half, 1) * sine


def turn_back(block, cosine, sine):
    half = block.shape[-1] // 2
    return block * cosine - pltpu.roll(block, half, 1) * sine


def first_kernel(slots, rows, inner, factor):
    def kernel(*refs):
        place, rate_ref, query, value, cosine, sine = refs[:6]
        cotans = refs[6 : 6 + slots]
        outs = refs[6 + slots :]
        grads, turned_grads = outs[:slots], outs[slots : 2 * slots]
        rotated, trailing, cotan, whole_grad, flat_grad = outs[2 * slots :]
        here = place[0]
        rate = rate_ref[pl.program_id(0)]
        for k in range(slots):
            cotan[pl.ds((here ^ k) * rows, rows), :] = cotans[k][...]
        _, flipped, rising, falling, whole = decays(rate, inner)
        seq_len = query.shape[0]
        carry = jnp.zeros((query.shape[1], value.shape[1]), jnp.float32)
        for n in reversed(range(seq_len // inner)):
            at = slice(n * inner, (n + 1) * inner)
            cos, sin = cosine[at, :], sine[at, :]
            turned = turn(query[at, :].astype(jnp.float32), cos, sin).astype(jnp.bfloat16)
            rotated[at, :] = turned
            co, va = cotan[at, :], value[at, :]
            mix = (dot(va, co, 1, 1) * flipped).astype(jnp.bfloat16)
            trail = carry.astype(jnp.bfloat16)
            trailing[0, n] = trail
            grad = dot(mix, turned, 1, 0) + falling * dot(va, trail, 1, 1)
            grad = turn_back(grad, cos, sin) * factor
            whole_grad[at, :] = grad.astype(jnp.bfloat16)
            start = n * inner % rows
            flat_grad[n * inner // rows, :, start : start + inner] = grad.T.astype(jnp.bfloat16)
            decayed = (turned.astype(jnp.float32) * rising).astype(jnp.bfloat16)
            carry = carry * whole + dot(decayed, co, 0, 0)
        for k in range(slots):
            grads[k][...] = whole_grad[pl.ds((here ^ k) * rows, rows), :]
            turned_grads[k][...] = flat_grad[here ^ k]

    return kernel


def second_kernel(slots, rows, inner, factor):
    def kernel(*refs):
        place, rate_ref, rotated, value, cosine, sine, trailing, keys = refs[:8]
        cotans = refs[8 : 8 + slots]
        grad_query, grad_value, cotan, key = refs[8 + slots :]
        here = place[0]
        rate = rate_ref[pl.program_id(0)]
        for k in range(slots):
            at = pl.ds((here ^ k) * rows, rows)
            cotan[at, :] = cotans[k][...]
            key[at, :] = keys[k * rows : (k + 1) * rows, :]
        within, flipped, rising, falling, whole = decays(rate, inner)
        seq_len = rotated.shape[0]
        carry = jnp.zeros((rotated.shape[1], value.shape[1]), jnp.float32)
        for n in range(seq_len // inner):
            at = slice(n * inner, (n + 1) * inner)
            cos, sin = cosine[at, :], sine[at, :]
            rk = (turn(key[at, :].astype(jnp.float32), cos, sin) * factor).astype(jnp.bfloat16)
            rq, co, va = rotated[at, :], cotan[at, :], value[at, :]
            score = (dot(rk, rq, 1, 1) * flipped).astype(jnp.bfloat16)
            entering = carry.astype(jnp.bfloat16)
            mix = (dot(co, va, 1, 1) * within).astype(jnp.bfloat16)
            grad = dot(mix, rk, 1, 0) + rising * dot(co, entering, 1, 1)
            grad_query[at, :] = turn_back(grad, cos, sin).astype(jnp.bfloat16)
            grad_value[at, :] = (
                dot(score, co, 1, 0) + falling * dot(rk, trailing[0, n], 1, 0)
            ).astype(jnp.bfloat16)
            decayed = (rk.astype(jnp.float32) * falling).astype(jnp.bfloat16)
            carry = carry * whole + dot(decayed, va, 0, 0)

    return kernel


def prefetch(*values):
    return jnp.stack([jnp.asarray(v, jnp.int32) for v in values])


def near(count=1):
    return [pl.BlockSpec(memory_space=pltpu.VMEM)] * count


def away(count=1):
    return [pl.BlockSpec(memory_space=pltpu.HBM)] * count


def smem():
    return pl.BlockSpec(memory_space=pltpu.SMEM)


def retention_first(here, rate, query, value, cosine, sine, cotans, key_width):
    slots = len(cotans)
    seq_len, query_width = query.shape
    heads = query_width // key_width
    value_width = value.shape[1] // heads
    rows = cotans[0].shape[0]
    inner = min(INNER, rows)
    nblocks = seq_len // inner
    half = jnp.bfloat16
    full = spec((seq_len, key_width), lambda h: (0, 0))
    head = spec((seq_len, key_width), lambda h: (0, h))
    outs = [pltpu.HBM((rows, query_width), half)] * slots
    outs += [pltpu.HBM((query_width, rows), half)] * slots
    outs += [
        pltpu.HBM((seq_len, query_width), half),
        pltpu.HBM((heads, nblocks, key_width, value_width), half),
    ]
    result = pl.pallas_call(
        first_kernel(slots, rows, inner, key_width**-0.5),
        grid=(heads,),
        in_specs=[smem(), smem(), head, spec((seq_len, value_width), lambda h: (0, h)), full, full]
        + [spec((rows, value_width), lambda h: (0, h))] * slots,
        out_specs=[spec((rows, key_width), lambda h: (0, h))] * slots
        + [spec((key_width, rows), lambda h: (h, 0))] * slots
        + [
            head,
            spec((1, nblocks, key_width, value_width), lambda h: (h, 0, 0, 0)),
        ],
        out_shape=outs,
        scratch_shapes=[
            pltpu.VMEM((seq_len, value_width), half),
            pltpu.VMEM((seq_len, key_width), half),
            pltpu.VMEM((slots, key_width, rows), half),
        ],
        compiler_params=limit(16),
        cost_estimate=cost(6e9, 10e6),
        name="retention_first",
    )(prefetch(here), rate, query, value, cosine, sine, *cotans)
    return list(result[:slots]), list(result[slots : 2 * slots]), *result[2 * slots :]


def retention_second(here, rate, rotated, value, cosine, sine, trailing, keys, cotans):
    slots = len(cotans)
    heads, nblocks, key_width, value_width = trailing.shape
    seq_len = rotated.shape[0]
    inner = seq_len // nblocks
    rows = cotans[0].shape[0]
    half = jnp.bfloat16
    full = spec((seq_len, key_width), lambda h: (0, 0))
    head = spec((seq_len, key_width), lambda h: (0, h))
    wide = spec((seq_len, value_width), lambda h: (0, h))
    return pl.pallas_call(
        second_kernel(slots, rows, inner, key_width**-0.5),
        grid=(heads,),
        in_specs=[
            smem(),
            smem(),
            head,
            wide,
            full,
            full,
            spec((1, nblocks, key_width, value_width), lambda h: (h, 0, 0, 0)),
            spec((slots * rows, key_width), lambda h: (0, h)),
        ]
        + [spec((rows, value_width), lambda h: (0, h))] * slots,
        out_specs=[head, wide],
        out_shape=[
            pltpu.HBM(rotated.shape, half),
            pltpu.HBM(value.shape, half),
        ],
        scratch_shapes=[
            pltpu.VMEM((seq_len, value_width), half),
            pltpu.VMEM((seq_len, key_width), half),
        ],
        compiler_params=limit(16),
        cost_estimate=cost(6e9, 14e6),
        name="retention_second",
    )(prefetch(here), rate, rotated, value, cosine, sine, trailing, keys, *cotans)


def halves(tokens):
    width = sum(part.shape[1] for part in tokens[0])
    found, place = ([], []), 0
    for k, parts in enumerate(tokens):
        for at, part in place_parts(parts):
            for piece in range(2 * part.shape[1] // width):
                found[2 * at // width + piece].append((k, place, piece))
            place += 1
    return found


def key_projection(here, plane, core, tokens, shards):
    slots = len(tokens)
    planes = len(shards)
    parts = [part for slot in tokens for part in slot]
    loads = halves(tokens)
    rows, width = tokens[0][0].shape[0], sum(part.shape[1] for part in tokens[0])
    share = shards[0][0].shape[0]
    half = width // 2

    def kernel(*refs):
        place = refs[0]
        token_refs = refs[1 : 1 + len(parts)]
        shard_refs = refs[1 + len(parts) : 1 + len(parts) + 2 * planes]
        out, weight, token, total, sems = refs[1 + len(parts) + 2 * planes :]
        slot, own = place[0], place[1]

        def weight_copy(r, side, at):
            return pltpu.make_async_copy(
                shard_refs[2 * r + side].at[:, at * half : (at + 1) * half],
                weight.at[at, pl.ds(pl.multiple_of((own ^ side) * share, share), share)],
                sems.at[at, slots + side],
            )

        def token_copy(at, k, index, piece):
            return pltpu.make_async_copy(
                token_refs[index].at[:, piece * half : (piece + 1) * half],
                token.at[at, k * rows : (k + 1) * rows],
                sems.at[at, k],
            )

        for at in range(2):
            for r in range(planes):

                @pl.when(slot == r)
                def _():
                    for side in range(2):
                        weight_copy(r, side, at).start()

            for k, index, piece in loads[at]:
                token_copy(at, k, index, piece).start()
        for at in range(2):
            for side in range(2):
                weight_copy(0, side, at).wait()
            for k, index, piece in loads[at]:
                token_copy(at, k, index, piece).wait()
            term = dot(token[at], weight[at], 1, 1)
            if at == 0:
                total[...] = term
            else:
                out[...] = (total[...] + term).astype(jnp.bfloat16)

    far = len(tokens[-1])
    return pl.pallas_call(
        kernel,
        in_specs=[smem()] + away(len(parts) - far) + near(far) + away(2 * planes),
        out_specs=near()[0],
        out_shape=pltpu.VMEM((slots * rows, 2 * share), jnp.bfloat16),
        scratch_shapes=[
            pltpu.VMEM((2, 2 * share, half), jnp.bfloat16),
            pltpu.VMEM((2, slots * rows, half), jnp.bfloat16),
            pltpu.VMEM((slots * rows, 2 * share), jnp.float32),
            pltpu.SemaphoreType.DMA((2, slots + 2)),
        ],
        compiler_params=limit(20),
        cost_estimate=cost(4e9, 8e6),
        name="key_projection",
    )(
        prefetch((plane - here) % planes, core),
        *parts,
        *[part for pair in shards for part in pair],
    )


def token_gradient(here, plane, core, grads, shards):
    slots = len(grads)
    planes = len(shards)
    rows = grads[0].shape[0]
    share, width = shards[0][0].shape

    def kernel(*refs):
        place = refs[0]
        grad_refs = refs[1 : 1 + slots]
        shard_refs = refs[1 + slots : 1 + slots + 2 * planes]
        out, grad, weight, total, sems = refs[1 + slots + 2 * planes :]
        own = place[2]

        def grad_copy(k):
            return pltpu.make_async_copy(grad_refs[k], grad.at[k], sems.at[2 * planes + k])

        def shard_copy(r, side):
            return pltpu.make_async_copy(
                shard_refs[2 * r + side], weight.at[r, own ^ side], sems.at[2 * r + side]
            )

        for k in range(slots):
            grad_copy(k).start()
        for r in range(planes):
            for side in range(2):
                shard_copy(r, side).start()
        for k in range(slots):
            grad_copy(k).wait()
        for r in range(planes):
            k = ((place[1] + planes - r) % planes) ^ place[0]
            for side in range(2):
                shard_copy(r, side).wait()
            block = grad[k]
            term = dot(block[:, :share], weight[r, 0], 1, 0)
            term += dot(block[:, share:], weight[r, 1], 1, 0)
            if r == 0:
                total[...] = term
            elif r < planes - 1:
                total[...] += term
            else:
                out[...] = (total[...] + term).astype(jnp.bfloat16)

    return pl.pallas_call(
        kernel,
        in_specs=[smem()] + away(slots + 2 * planes),
        out_specs=near()[0],
        out_shape=jax.ShapeDtypeStruct((rows, width), jnp.bfloat16),
        scratch_shapes=[
            pltpu.VMEM((slots, rows, 2 * share), jnp.bfloat16),
            pltpu.VMEM((planes, 2, share, width), jnp.bfloat16),
            pltpu.VMEM((rows, width), jnp.float32),
            pltpu.SemaphoreType.DMA((2 * planes + slots,)),
        ],
        compiler_params=limit(20),
        cost_estimate=cost(5e9, 11e6),
        name="token_gradient",
    )(prefetch(here, plane, core), *grads, *[part for pair in shards for part in pair])


def place_parts(parts):
    at, placed = 0, []
    for part in parts:
        placed.append((at, part))
        at += part.shape[1]
    return placed


def weight_start(grads, tokens):
    slots = len(tokens)
    features, rows = grads[0].shape
    parts = [part for slot in tokens for part in slot]
    loads = halves(tokens)
    width = sum(part.shape[1] for part in tokens[0])
    half = width // 2

    def kernel(*refs):
        grad_refs, token_refs = refs[: slots + 1], refs[slots + 1 : slots + 1 + len(parts)]
        out, last, grad, token, sems, grad_sems = refs[slots + 1 + len(parts) :]

        def fetch(at, k, index, piece):
            return pltpu.make_async_copy(
                token_refs[index].at[:, piece * half : (piece + 1) * half],
                token.at[at, k],
                sems.at[at, k],
            )

        def fetch_grad(k):
            to = grad.at[k] if k < slots else last
            return pltpu.make_async_copy(grad_refs[k], to, grad_sems.at[k])

        for k in range(slots):
            fetch_grad(k).start()
        for at in range(2):
            for load in loads[at]:
                fetch(at, *load).start()
        fetch_grad(slots).start()
        for k in range(slots):
            fetch_grad(k).wait()
        for at in range(2):
            for load in loads[at]:
                fetch(at, *load).wait()
            total = dot(grad[0], token[at, 0], 1, 0)
            for k in range(1, slots):
                total += dot(grad[k], token[at, k], 1, 0)
            out[:, at * half : (at + 1) * half] = total
        fetch_grad(slots).wait()

    return pl.pallas_call(
        kernel,
        in_specs=away(slots + 1 + len(parts)),
        out_specs=near(2),
        out_shape=[
            pltpu.VMEM((features, width), jnp.float32),
            pltpu.VMEM((features, rows), jnp.bfloat16),
        ],
        scratch_shapes=[
            pltpu.VMEM((slots, features, rows), jnp.bfloat16),
            pltpu.VMEM((2, slots, rows, half), jnp.bfloat16),
            pltpu.SemaphoreType.DMA((2, slots)),
            pltpu.SemaphoreType.DMA((slots + 1,)),
        ],
        compiler_params=limit(20),
        cost_estimate=cost(4e9, 6e6),
        name="weight_start",
    )(*grads, *parts)


def weight_end(side, grad, tokens, total, kind):
    features, width = total.shape
    share = features // 2

    def kernel(place, grad_ref, *refs):
        token_refs, (so_far, out) = refs[: len(tokens)], refs[len(tokens) :]
        rows = pl.ds(pl.multiple_of(place[0] * share, share), share)
        for (at, part), ref in zip(place_parts(tokens), token_refs):
            to = slice(at, at + part.shape[1])
            term = dot(grad_ref[rows, :], ref[...], 1, 0)
            out[:, to] = (so_far[rows, to] + term).astype(kind)

    return pl.pallas_call(
        kernel,
        in_specs=[smem()] + near(2 + len(tokens)),
        out_specs=near()[0],
        out_shape=pltpu.VMEM((share, width), kind),
        compiler_params=limit(20),
        cost_estimate=cost(2e9, 6e6),
        name="weight_end",
    )(prefetch(side), grad, *tokens, total)


def weight_pieces(here, slots, chunks, kept, received):
    share, width = kept.shape
    tile = width // slots
    size = tile // chunks

    def kernel(place, own, other, *outs):
        for k in range(slots):
            for chunk in range(chunks):
                start = pl.multiple_of((place[0] ^ k) * tile + chunk * size, size)
                at = pl.ds(start, size)
                total = own[:, at] + other[:, at].astype(jnp.float32)
                outs[chunk * slots + k][...] = total.astype(jnp.bfloat16)

    result = pl.pallas_call(
        kernel,
        in_specs=[smem()] + near(2),
        out_specs=near(slots * chunks),
        out_shape=([pltpu.HBM((share, size), jnp.bfloat16)] + [pltpu.VMEM((share, size), jnp.bfloat16)] * (slots - 1)) * chunks,
        compiler_params=limit(12),
        cost_estimate=cost(2e9, 6e6),
        name="weight_pieces",
    )(prefetch(here), kept, received)
    return [result[chunk * slots : (chunk + 1) * slots] for chunk in range(chunks)]


def route(here, plane, planes, pieces):
    slots = len(pieces)
    shape = pieces[0].shape

    def kernel(place, *refs):
        outs, (stack, sem) = refs[slots:-2], refs[-2:]
        own = pltpu.make_async_copy(refs[0], stack.at[0], sem)
        own.start()
        for k in range(1, slots):
            stack[k] = refs[k][...]
        own.wait()
        for k in range(planes):
            outs[k][...] = stack[place[0] ^ place[1] ^ k]

    return pl.pallas_call(
        kernel,
        in_specs=[smem()] + away() + near(slots - 1),
        out_specs=near(planes),
        out_shape=[pltpu.VMEM(shape, jnp.bfloat16)] * planes,
        scratch_shapes=[pltpu.VMEM((slots, *shape), jnp.bfloat16), pltpu.SemaphoreType.DMA],
        compiler_params=limit(12),
        cost_estimate=cost(1e9, 2e6),
        name="route",
    )(prefetch(here, plane), *pieces)


def add_up(groups):
    count, (rows, size) = len(groups[0]), groups[0][0].shape

    def kernel(*refs):
        for side in range(len(groups)):
            terms = refs[side * count : (side + 1) * count]
            total = terms[0][...].astype(jnp.float32)
            for ref in terms[1:]:
                total += ref[...].astype(jnp.float32)
            refs[-1][:, side * size : (side + 1) * size] = total.astype(jnp.bfloat16)

    return pl.pallas_call(
        kernel,
        in_specs=near(count * len(groups)),
        out_specs=near()[0],
        out_shape=pltpu.VMEM((rows, size * len(groups)), jnp.bfloat16),
        compiler_params=limit(12),
        cost_estimate=cost(1e9, 1e6),
        name="add_up",
    )(*[term for group in groups for term in group])


def lay_out(here, pieces):
    slots = len(pieces)
    share, size = pieces[0].shape

    def kernel(place, *refs):
        out, wide, sems = refs[slots:]

        def store(k):
            at = pl.ds(pl.multiple_of((place[0] ^ k) * size, size), size)
            return pltpu.make_async_copy(wide.at[k], out.at[:, at], sems.at[k])

        for k in range(slots):
            wide[k] = refs[k][...].astype(jnp.float32)
            store(k).start()
        for k in range(slots):
            store(k).wait()

    return pl.pallas_call(
        kernel,
        in_specs=[smem()] + near(slots),
        out_specs=away()[0],
        out_shape=jax.ShapeDtypeStruct((share, size * slots), jnp.float32),
        scratch_shapes=[
            pltpu.VMEM((slots, share, size), jnp.float32),
            pltpu.SemaphoreType.DMA((slots,)),
        ],
        compiler_params=limit(12),
        cost_estimate=cost(1e9, 4e6),
        name="lay_out",
    )(prefetch(here), *pieces)


def gather_slots(array):
    half = array.shape[1] // 2
    low, high = array[:, :half], array[:, half:]
    near_high, next_low = swap(high, "sp", 1), swap(low, "sp", 2)
    near_low, next_high = swap(low, "sp", 1), swap(high, "sp", 2)
    far = [swap(next_low, "sp", 1), swap(near_high, "sp", 2)]
    return [[array], [near_low, near_high], [next_low, next_high], far]


def direct_body(tokens, key_weight, queries, values, cotangent, log_decay):
    return direct_steps(tokens, key_weight, queries, values, cotangent, log_decay)


def direct_steps(tokens, key_weight, queries, values, cotangent, log_decay):
    here, member = lax.axis_index("sp"), lax.axis_index("dp")
    slots = lax.axis_size("sp")
    planes = lax.axis_size("dp") // 2
    plane, core = member // 2, member % 2
    seq_len, heads, key_width = queries.shape[1:]
    value_width = values.shape[3]
    rate = lax.dynamic_slice_in_dim(log_decay, here * heads, heads)
    cosine, sine = rotation(seq_len, key_width // 2)
    cosine, sine = cosine[:, 0], sine[:, 0]
    cosine = jnp.concatenate([cosine, cosine], axis=1)
    sine = jnp.concatenate([-sine, sine], axis=1)

    ring = [key_weight]
    for _ in range(1, planes):
        ring.append(step_planes(ring[-1]))
    shards = [(part, swap(part, "dp", 1)) for part in ring]

    cotans = [columns(cotangent[0], here ^ k, heads * value_width) for k in range(slots)]
    cotans = cotans[:1] + [swap(cotans[k], "sp", k) for k in range(1, slots)]
    token_slots = gather_slots(tokens[0])

    query = queries[0].reshape(seq_len, heads * key_width)
    value = values[0].reshape(seq_len, heads * value_width)
    grads, turned_grads, rotated, trailing = retention_first(
        here, rate, query, value, cosine, sine, cotans, key_width
    )

    total, last = weight_start(turned_grads, token_slots[:-1])
    sent = weight_end(core ^ 1, last, token_slots[-1], total, jnp.bfloat16)
    received = swap(sent, "dp", 1)
    kept = weight_end(core, last, token_slots[-1], total, jnp.float32)
    chunks = weight_pieces(here, slots, CHUNKS, kept, received)
    groups = []
    for pieces in chunks:
        came = [pieces[0]] + [swap(pieces[k], "sp", k) for k in range(1, slots)]
        terms = route(here, plane, planes, came)
        others = [swap(terms[k], "dp", 2 * k) for k in range(1, planes)]
        groups.append([terms[0]] + others)
    total = add_up(groups)
    gathered = [total] + [swap(total, "sp", k) for k in range(1, slots)]
    grad_weight = lay_out(here, gathered)

    returned = [grads[0]] + [swap(grads[k], "sp", k) for k in range(1, slots)]
    grad_tokens = token_gradient(here, plane, core, returned, shards)

    keys = key_projection(here, plane, core, token_slots, shards)
    grad_query, grad_value = retention_second(
        here, rate, rotated, value, cosine, sine, trailing, keys, cotans
    )
    grad_query = grad_query.reshape(queries.shape)
    grad_value = grad_value.reshape(values.shape)
    return (
        grad_tokens[None],
        grad_query,
        grad_value,
        grad_weight,
    )


def solution(mesh):
    slots, members = mesh.shape["sp"], mesh.shape["dp"]
    direct = members == 2 * slots and slots == 4
    return jax.shard_map(
        direct_body if direct else general_body,
        mesh=mesh,
        in_specs=(
            P("dp", "sp", None),
            P("dp", None),
            P("dp", None, "sp", None),
            P("dp", None, "sp", None),
            P("dp", "sp", None),
            P(),
        ),
        out_specs=(
            P("dp", "sp", None),
            P("dp", None, "sp", None),
            P("dp", None, "sp", None),
            P("dp", None),
        ),
        check_vma=False,
    )
```

```python
import jax
import jax.numpy as jnp
from jax import lax
from jax.experimental import pallas as pl
from jax.experimental.pallas import tpu as pltpu
from jax.sharding import PartitionSpec as P

BLOCK = 128


def product(form, left, right):
    return jnp.einsum(form, left, right, preferred_element_type=jnp.float32)


def rotation(seq_len, half):
    position = jnp.arange(seq_len, dtype=jnp.float32)
    frequency = 10000.0 ** (-jnp.arange(half, dtype=jnp.float32) / half)
    angle = position[:, None] * frequency[None, :]
    return (jnp.cos(angle)[:, None, :], jnp.sin(angle)[:, None, :])


def rotate(vectors, cosine, sine):
    half = vectors.shape[-1] // 2
    front, back = (vectors[..., :half], vectors[..., half:])
    return jnp.concatenate([front * cosine - back * sine, front * sine + back * cosine], axis=-1)


def unrotate(grads, cosine, sine):
    half = grads.shape[-1] // 2
    front, back = (grads[..., :half], grads[..., half:])
    return jnp.concatenate([front * cosine + back * sine, back * cosine - front * sine], axis=-1)


def retention_backward(query_rows, key_rows, value_rows, cotan_rows, head_decay):
    seq_len, heads_here, key_width = query_rows.shape
    nblocks = seq_len // BLOCK
    cosine, sine = rotation(seq_len, key_width // 2)
    factor = key_width ** (-0.5)
    rot_query = rotate(query_rows.astype(jnp.float32), cosine, sine).astype(jnp.bfloat16)
    rot_key = (rotate(key_rows.astype(jnp.float32), cosine, sine) * factor).astype(jnp.bfloat16)

    def blocks(array):
        return array.reshape(nblocks, BLOCK, heads_here, array.shape[-1])

    block_query, block_key = (blocks(rot_query), blocks(rot_key))
    block_value, block_cotan = (blocks(value_rows), blocks(cotan_rows))
    inside = jnp.arange(BLOCK, dtype=jnp.float32)
    offset = inside[:, None] - inside[None, :]
    within = jnp.where(
        offset[None] >= 0, jnp.exp(jnp.maximum(offset, 0.0)[None] * head_decay[:, None, None]), 0.0
    )
    rising = jnp.exp((inside + 1.0)[:, None] * head_decay[None, :])[None, :, :, None]
    falling = jnp.exp((BLOCK - 1.0 - inside)[:, None] * head_decay[None, :])[None, :, :, None]
    scores = (product("nihd,njhd->nhij", block_query, block_key) * within[None]).astype(
        jnp.bfloat16
    )
    mixing = (product("nihe,njhe->nhij", block_cotan, block_value) * within[None]).astype(
        jnp.bfloat16
    )
    decayed_queries = (block_query.astype(jnp.float32) * rising).astype(jnp.bfloat16)
    decayed_keys = (block_key.astype(jnp.float32) * falling).astype(jnp.bfloat16)
    block_states = product("nihd,nihe->nhde", decayed_keys, block_value)
    block_trails = product("nihd,nihe->nhde", decayed_queries, block_cotan)
    block_index = jnp.arange(nblocks, dtype=jnp.float32)
    spacing = block_index[:, None] - block_index[None, :] - 1.0
    earlier = jnp.where(
        spacing[None] >= 0,
        jnp.exp(jnp.maximum(spacing, 0.0)[None] * BLOCK * head_decay[:, None, None]),
        0.0,
    )
    later = jnp.transpose(earlier, (0, 2, 1))
    entering = jnp.einsum(
        "hnm,mhde->nhde", earlier, block_states, precision=lax.Precision.HIGHEST
    ).astype(jnp.bfloat16)
    trailing = jnp.einsum(
        "hnm,mhde->nhde", later, block_trails, precision=lax.Precision.HIGHEST
    ).astype(jnp.bfloat16)
    grad_rq = product("nhij,njhd->nihd", mixing, block_key) + rising * product(
        "nihe,nhde->nihd", block_cotan, entering
    )
    grad_rk = product("nhij,nihd->njhd", mixing, block_query) + falling * product(
        "nihe,nhde->nihd", block_value, trailing
    )
    grad_value = product("nhij,nihe->njhe", scores, block_cotan) + falling * product(
        "nihd,nhde->nihe", block_key, trailing
    )
    grad_rq = grad_rq.reshape(seq_len, heads_here, key_width)
    grad_rk = grad_rk.reshape(seq_len, heads_here, key_width)
    grad_query = unrotate(grad_rq, cosine, sine).astype(jnp.bfloat16)
    grad_key = (unrotate(grad_rk, cosine, sine) * factor).astype(jnp.bfloat16)
    grad_value = grad_value.reshape(seq_len, heads_here, -1).astype(jnp.bfloat16)
    return (grad_query, grad_key, grad_value)


def general_body(tokens, key_weight, queries, values, cotangent, log_decay):
    gathered = lax.all_gather(key_weight, "dp", axis=0, tiled=True)
    token_rows = tokens[0]
    key_proj = jnp.einsum(
        "td,qd->tq", token_rows, gathered, preferred_element_type=jnp.float32
    ).astype(jnp.bfloat16)
    head_keys, head_cotan = (
        lax.all_to_all(key_proj[None], "sp", split_axis=2, concat_axis=1, tiled=True),
        lax.all_to_all(cotangent, "sp", split_axis=2, concat_axis=1, tiled=True),
    )
    seq_len = head_keys.shape[1]
    heads_here = queries.shape[2]
    head_start = lax.axis_index("sp") * heads_here
    head_decay = lax.dynamic_slice_in_dim(log_decay, head_start, heads_here)
    grad_query, grad_key, grad_value = retention_backward(
        queries[0],
        head_keys[0].reshape(seq_len, heads_here, -1),
        values[0],
        head_cotan[0].reshape(seq_len, heads_here, -1),
        head_decay,
    )
    returned = lax.all_to_all(
        grad_key.reshape(1, seq_len, -1), "sp", split_axis=1, concat_axis=2, tiled=True
    )
    key_grads = returned[0]
    grad_tokens = jnp.dot(key_grads, gathered, preferred_element_type=jnp.float32).astype(
        jnp.bfloat16
    )
    width = key_grads.shape[1]
    count_dp = lax.axis_size("dp")
    count_sp = lax.axis_size("sp")
    share = width // (count_sp * count_dp)
    ordered = (
        key_grads.reshape(-1, count_dp, count_sp, share).transpose(0, 2, 1, 3).reshape(-1, width)
    )
    partial_grad = jnp.einsum("tq,td->qd", ordered, token_rows, preferred_element_type=jnp.float32)
    owned = lax.psum_scatter(partial_grad, ("sp", "dp"), scatter_dimension=0, tiled=True)
    weight_grad = lax.all_gather(owned, "sp", axis=0, tiled=True)
    return (grad_tokens[None], grad_query[None], grad_value[None], weight_grad)


INNER = 256
CHUNKS = 2


def swap(array, axis, bit):
    count = lax.axis_size(axis)
    return lax.ppermute(array, axis, [(i, i ^ bit) for i in range(count)])


def step_planes(array):
    count = lax.axis_size("dp")
    return lax.ppermute(array, "dp", [(i, (i + 2) % count) for i in range(count)])


def limit(mib):
    return pltpu.CompilerParams(vmem_limit_bytes=mib * 2**20)


def dot(left, right, left_dim, right_dim):
    return lax.dot_general(
        left, right, (((left_dim,), (right_dim,)), ((), ())), preferred_element_type=jnp.float32
    )


def columns(array, index, width):
    return lax.dynamic_slice_in_dim(array, index * width, width, axis=1)


def cost(flops, moved):
    return pl.CostEstimate(flops=int(flops), bytes_accessed=int(moved), transcendentals=0)


def spec(shape, index):
    return pl.BlockSpec(shape, index)


def decays(rate, size):
    rows = lax.broadcasted_iota(jnp.int32, (size, size), 0)
    cols = lax.broadcasted_iota(jnp.int32, (size, size), 1)
    gap = (rows - cols).astype(jnp.float32)
    within = jnp.where(gap >= 0, jnp.exp(jnp.maximum(gap, 0.0) * rate), 0.0)
    flipped = jnp.where(gap <= 0, jnp.exp(jnp.maximum(-gap, 0.0) * rate), 0.0)
    place = lax.broadcasted_iota(jnp.int32, (size, 1), 0).astype(jnp.float32)
    rising = jnp.exp((place + 1.0) * rate)
    falling = jnp.exp((size - 1.0 - place) * rate)
    whole = jnp.exp(jnp.full((1, 1), float(size), jnp.float32) * rate)
    return within, flipped, rising, falling, whole


def turn(block, cosine, sine):
    half = block.shape[-1] // 2
    return block * cosine + pltpu.roll(block, half, 1) * sine


def turn_back(block, cosine, sine):
    half = block.shape[-1] // 2
    return block * cosine - pltpu.roll(block, half, 1) * sine


def first_kernel(slots, rows, inner, factor):
    def kernel(*refs):
        place, rate_ref, query, value, cosine, sine = refs[:6]
        cotans = refs[6 : 6 + slots]
        outs = refs[6 + slots :]
        grads, turned_grads = outs[:slots], outs[slots : 2 * slots]
        rotated, trailing, cotan, whole_grad, flat_grad = outs[2 * slots :]
        here = place[0]
        rate = rate_ref[pl.program_id(0)]
        for k in range(slots):
            cotan[pl.ds((here ^ k) * rows, rows), :] = cotans[k][...]
        _, flipped, rising, falling, whole = decays(rate, inner)
        seq_len = query.shape[0]
        carry = jnp.zeros((query.shape[1], value.shape[1]), jnp.float32)
        for n in reversed(range(seq_len // inner)):
            at = slice(n * inner, (n + 1) * inner)
            cos, sin = cosine[at, :], sine[at, :]
            turned = turn(query[at, :].astype(jnp.float32), cos, sin).astype(jnp.bfloat16)
            rotated[at, :] = turned
            co, va = cotan[at, :], value[at, :]
            mix = (dot(va, co, 1, 1) * flipped).astype(jnp.bfloat16)
            trail = carry.astype(jnp.bfloat16)
            trailing[0, n] = trail
            grad = dot(mix, turned, 1, 0) + falling * dot(va, trail, 1, 1)
            grad = turn_back(grad, cos, sin) * factor
            whole_grad[at, :] = grad.astype(jnp.bfloat16)
            start = n * inner % rows
            flat_grad[n * inner // rows, :, start : start + inner] = grad.T.astype(jnp.bfloat16)
            decayed = (turned.astype(jnp.float32) * rising).astype(jnp.bfloat16)
            carry = carry * whole + dot(decayed, co, 0, 0)
        for k in range(slots):
            grads[k][...] = whole_grad[pl.ds((here ^ k) * rows, rows), :]
            turned_grads[k][...] = flat_grad[here ^ k]

    return kernel


def second_kernel(slots, rows, inner, factor):
    def kernel(*refs):
        place, rate_ref, rotated, value, cosine, sine, trailing, keys = refs[:8]
        cotans = refs[8 : 8 + slots]
        grad_query, grad_value, cotan, key = refs[8 + slots :]
        here = place[0]
        rate = rate_ref[pl.program_id(0)]
        for k in range(slots):
            at = pl.ds((here ^ k) * rows, rows)
            cotan[at, :] = cotans[k][...]
            key[at, :] = keys[k * rows : (k + 1) * rows, :]
        within, flipped, rising, falling, whole = decays(rate, inner)
        seq_len = rotated.shape[0]
        carry = jnp.zeros((rotated.shape[1], value.shape[1]), jnp.float32)
        for n in range(seq_len // inner):
            at = slice(n * inner, (n + 1) * inner)
            cos, sin = cosine[at, :], sine[at, :]
            rk = (turn(key[at, :].astype(jnp.float32), cos, sin) * factor).astype(jnp.bfloat16)
            rq, co, va = rotated[at, :], cotan[at, :], value[at, :]
            score = (dot(rk, rq, 1, 1) * flipped).astype(jnp.bfloat16)
            entering = carry.astype(jnp.bfloat16)
            mix = (dot(co, va, 1, 1) * within).astype(jnp.bfloat16)
            grad = dot(mix, rk, 1, 0) + rising * dot(co, entering, 1, 1)
            grad_query[at, :] = turn_back(grad, cos, sin).astype(jnp.bfloat16)
            grad_value[at, :] = (
                dot(score, co, 1, 0) + falling * dot(rk, trailing[0, n], 1, 0)
            ).astype(jnp.bfloat16)
            decayed = (rk.astype(jnp.float32) * falling).astype(jnp.bfloat16)
            carry = carry * whole + dot(decayed, va, 0, 0)

    return kernel


def prefetch(*values):
    return jnp.stack([jnp.asarray(v, jnp.int32) for v in values])


def near(count=1):
    return [pl.BlockSpec(memory_space=pltpu.VMEM)] * count


def away(count=1):
    return [pl.BlockSpec(memory_space=pltpu.HBM)] * count


def smem():
    return pl.BlockSpec(memory_space=pltpu.SMEM)


def retention_first(here, rate, query, value, cosine, sine, cotans, key_width):
    slots = len(cotans)
    seq_len, query_width = query.shape
    heads = query_width // key_width
    value_width = value.shape[1] // heads
    rows = cotans[0].shape[0]
    inner = min(INNER, rows)
    nblocks = seq_len // inner
    half = jnp.bfloat16
    full = spec((seq_len, key_width), lambda h: (0, 0))
    head = spec((seq_len, key_width), lambda h: (0, h))
    outs = [pltpu.HBM((rows, query_width), half)] * slots
    outs += [pltpu.VMEM((query_width, rows), half)] * slots
    outs += [
        pltpu.HBM((seq_len, query_width), half),
        pltpu.HBM((heads, nblocks, key_width, value_width), half),
    ]
    result = pl.pallas_call(
        first_kernel(slots, rows, inner, key_width**-0.5),
        grid=(heads,),
        in_specs=[smem(), smem(), head, spec((seq_len, value_width), lambda h: (0, h)), full, full]
        + [spec((rows, value_width), lambda h: (0, h))] * slots,
        out_specs=[spec((rows, key_width), lambda h: (0, h))] * slots
        + [spec((key_width, rows), lambda h: (h, 0))] * slots
        + [
            head,
            spec((1, nblocks, key_width, value_width), lambda h: (h, 0, 0, 0)),
        ],
        out_shape=outs,
        scratch_shapes=[
            pltpu.VMEM((seq_len, value_width), half),
            pltpu.VMEM((seq_len, key_width), half),
            pltpu.VMEM((slots, key_width, rows), half),
        ],
        compiler_params=limit(16),
        cost_estimate=cost(6e9, 10e6),
        name="retention_first",
    )(prefetch(here), rate, query, value, cosine, sine, *cotans)
    return list(result[:slots]), list(result[slots : 2 * slots]), *result[2 * slots :]


def retention_second(here, rate, rotated, value, cosine, sine, trailing, keys, cotans):
    slots = len(cotans)
    heads, nblocks, key_width, value_width = trailing.shape
    seq_len = rotated.shape[0]
    inner = seq_len // nblocks
    rows = cotans[0].shape[0]
    half = jnp.bfloat16
    full = spec((seq_len, key_width), lambda h: (0, 0))
    head = spec((seq_len, key_width), lambda h: (0, h))
    wide = spec((seq_len, value_width), lambda h: (0, h))
    return pl.pallas_call(
        second_kernel(slots, rows, inner, key_width**-0.5),
        grid=(heads,),
        in_specs=[
            smem(),
            smem(),
            head,
            wide,
            full,
            full,
            spec((1, nblocks, key_width, value_width), lambda h: (h, 0, 0, 0)),
            spec((slots * rows, key_width), lambda h: (0, h)),
        ]
        + [spec((rows, value_width), lambda h: (0, h))] * slots,
        out_specs=[head, wide],
        out_shape=[
            pltpu.HBM(rotated.shape, half),
            pltpu.HBM(value.shape, half),
        ],
        scratch_shapes=[
            pltpu.VMEM((seq_len, value_width), half),
            pltpu.VMEM((seq_len, key_width), half),
        ],
        compiler_params=limit(16),
        cost_estimate=cost(6e9, 14e6),
        name="retention_second",
    )(prefetch(here), rate, rotated, value, cosine, sine, trailing, keys, *cotans)


def halves(tokens):
    width = sum(part.shape[1] for part in tokens[0])
    found, place = ([], []), 0
    for k, parts in enumerate(tokens):
        for at, part in place_parts(parts):
            for piece in range(2 * part.shape[1] // width):
                found[2 * at // width + piece].append((k, place, piece))
            place += 1
    return found


def key_projection(here, plane, core, tokens, shards):
    slots = len(tokens)
    planes = len(shards)
    parts = [part for slot in tokens for part in slot]
    loads = halves(tokens)
    rows, width = tokens[0][0].shape[0], sum(part.shape[1] for part in tokens[0])
    share = shards[0][0].shape[0]
    half = width // 2

    def kernel(*refs):
        place = refs[0]
        token_refs = refs[1 : 1 + len(parts)]
        shard_refs = refs[1 + len(parts) : 1 + len(parts) + 2 * planes]
        out, weight, token, total, sems = refs[1 + len(parts) + 2 * planes :]
        slot, own = place[0], place[1]

        def weight_copy(r, side, at):
            return pltpu.make_async_copy(
                shard_refs[2 * r + side].at[:, at * half : (at + 1) * half],
                weight.at[at, pl.ds(pl.multiple_of((own ^ side) * share, share), share)],
                sems.at[at, slots + side],
            )

        def token_copy(at, k, index, piece):
            return pltpu.make_async_copy(
                token_refs[index].at[:, piece * half : (piece + 1) * half],
                token.at[at, k * rows : (k + 1) * rows],
                sems.at[at, k],
            )

        for at in range(2):
            for r in range(planes):

                @pl.when(slot == r)
                def _():
                    for side in range(2):
                        weight_copy(r, side, at).start()

            for k, index, piece in loads[at]:
                token_copy(at, k, index, piece).start()
        for at in range(2):
            for side in range(2):
                weight_copy(0, side, at).wait()
            for k, index, piece in loads[at]:
                token_copy(at, k, index, piece).wait()
            term = dot(token[at], weight[at], 1, 1)
            if at == 0:
                total[...] = term
            else:
                out[...] = (total[...] + term).astype(jnp.bfloat16)

    far = len(tokens[-1])
    return pl.pallas_call(
        kernel,
        in_specs=[smem()] + away(len(parts) - far) + near(far) + away(2 * planes),
        out_specs=near()[0],
        out_shape=pltpu.VMEM((slots * rows, 2 * share), jnp.bfloat16),
        scratch_shapes=[
            pltpu.VMEM((2, 2 * share, half), jnp.bfloat16),
            pltpu.VMEM((2, slots * rows, half), jnp.bfloat16),
            pltpu.VMEM((slots * rows, 2 * share), jnp.float32),
            pltpu.SemaphoreType.DMA((2, slots + 2)),
        ],
        compiler_params=limit(20),
        cost_estimate=cost(4e9, 8e6),
        name="key_projection",
    )(
        prefetch((plane - here) % planes, core),
        *parts,
        *[part for pair in shards for part in pair],
    )


def token_gradient(here, plane, core, grads, shards):
    slots = len(grads)
    planes = len(shards)
    rows = grads[0].shape[0]
    share, width = shards[0][0].shape

    def kernel(*refs):
        place = refs[0]
        grad_refs = refs[1 : 1 + slots]
        shard_refs = refs[1 + slots : 1 + slots + 2 * planes]
        out, grad, weight, total, sems = refs[1 + slots + 2 * planes :]
        own = place[2]

        def grad_copy(k):
            return pltpu.make_async_copy(grad_refs[k], grad.at[k], sems.at[2 * planes + k])

        def shard_copy(r, side):
            return pltpu.make_async_copy(
                shard_refs[2 * r + side], weight.at[r, own ^ side], sems.at[2 * r + side]
            )

        for k in range(slots):
            grad_copy(k).start()
        for r in range(planes):
            for side in range(2):
                shard_copy(r, side).start()
        for k in range(slots):
            grad_copy(k).wait()
        for r in range(planes):
            k = ((place[1] + planes - r) % planes) ^ place[0]
            for side in range(2):
                shard_copy(r, side).wait()
            block = grad[k]
            term = dot(block[:, :share], weight[r, 0], 1, 0)
            term += dot(block[:, share:], weight[r, 1], 1, 0)
            if r == 0:
                total[...] = term
            elif r < planes - 1:
                total[...] += term
            else:
                out[...] = (total[...] + term).astype(jnp.bfloat16)

    return pl.pallas_call(
        kernel,
        in_specs=[smem()] + away(slots + 2 * planes),
        out_specs=near()[0],
        out_shape=jax.ShapeDtypeStruct((rows, width), jnp.bfloat16),
        scratch_shapes=[
            pltpu.VMEM((slots, rows, 2 * share), jnp.bfloat16),
            pltpu.VMEM((planes, 2, share, width), jnp.bfloat16),
            pltpu.VMEM((rows, width), jnp.float32),
            pltpu.SemaphoreType.DMA((2 * planes + slots,)),
        ],
        compiler_params=limit(20),
        cost_estimate=cost(5e9, 11e6),
        name="token_gradient",
    )(prefetch(here, plane, core), *grads, *[part for pair in shards for part in pair])


def place_parts(parts):
    at, placed = 0, []
    for part in parts:
        placed.append((at, part))
        at += part.shape[1]
    return placed


def weight_start(grads, tokens):
    slots = len(tokens)
    features, rows = grads[0].shape
    parts = [part for slot in tokens for part in slot]
    loads = halves(tokens)
    width = sum(part.shape[1] for part in tokens[0])
    half = width // 2

    def kernel(*refs):
        grad_refs, token_refs = refs[:slots], refs[slots : slots + len(parts)]
        out, token, sems = refs[slots + len(parts) :]

        def fetch(at, k, index, piece):
            return pltpu.make_async_copy(
                token_refs[index].at[:, piece * half : (piece + 1) * half],
                token.at[at, k],
                sems.at[at, k],
            )

        for at in range(2):
            for load in loads[at]:
                fetch(at, *load).start()
        for at in range(2):
            for load in loads[at]:
                fetch(at, *load).wait()
            total = dot(grad_refs[0][...], token[at, 0], 1, 0)
            for k in range(1, slots):
                total += dot(grad_refs[k][...], token[at, k], 1, 0)
            out[:, at * half : (at + 1) * half] = total

    return pl.pallas_call(
        kernel,
        in_specs=near(slots) + away(len(parts)),
        out_specs=near()[0],
        out_shape=pltpu.VMEM((features, width), jnp.float32),
        scratch_shapes=[
            pltpu.VMEM((2, slots, rows, half), jnp.bfloat16),
            pltpu.SemaphoreType.DMA((2, slots)),
        ],
        compiler_params=limit(20),
        cost_estimate=cost(4e9, 6e6),
        name="weight_start",
    )(*grads, *parts)


def weight_end(side, grad, tokens, total, kind):
    features, width = total.shape
    share = features // 2

    def kernel(place, grad_ref, *refs):
        token_refs, (so_far, out) = refs[: len(tokens)], refs[len(tokens) :]
        rows = pl.ds(pl.multiple_of(place[0] * share, share), share)
        for (at, part), ref in zip(place_parts(tokens), token_refs):
            to = slice(at, at + part.shape[1])
            term = dot(grad_ref[rows, :], ref[...], 1, 0)
            out[:, to] = (so_far[rows, to] + term).astype(kind)

    return pl.pallas_call(
        kernel,
        in_specs=[smem()] + near(2 + len(tokens)),
        out_specs=near()[0],
        out_shape=pltpu.VMEM((share, width), kind),
        compiler_params=limit(20),
        cost_estimate=cost(2e9, 6e6),
        name="weight_end",
    )(prefetch(side), grad, *tokens, total)


def weight_pieces(here, slots, chunks, kept, received):
    share, width = kept.shape
    tile = width // slots
    size = tile // chunks

    def kernel(place, own, other, *outs):
        for k in range(slots):
            for chunk in range(chunks):
                start = pl.multiple_of((place[0] ^ k) * tile + chunk * size, size)
                at = pl.ds(start, size)
                total = own[:, at] + other[:, at].astype(jnp.float32)
                outs[chunk * slots + k][...] = total.astype(jnp.bfloat16)

    result = pl.pallas_call(
        kernel,
        in_specs=[smem()] + near(2),
        out_specs=near(slots * chunks),
        out_shape=([pltpu.HBM((share, size), jnp.bfloat16)] + [pltpu.VMEM((share, size), jnp.bfloat16)] * (slots - 1)) * chunks,
        compiler_params=limit(12),
        cost_estimate=cost(2e9, 6e6),
        name="weight_pieces",
    )(prefetch(here), kept, received)
    return [result[chunk * slots : (chunk + 1) * slots] for chunk in range(chunks)]


def route(here, plane, planes, pieces):
    slots = len(pieces)
    shape = pieces[0].shape

    def kernel(place, *refs):
        outs, (stack, sem) = refs[slots:-2], refs[-2:]
        own = pltpu.make_async_copy(refs[0], stack.at[0], sem)
        own.start()
        for k in range(1, slots):
            stack[k] = refs[k][...]
        own.wait()
        for k in range(planes):
            outs[k][...] = stack[place[0] ^ place[1] ^ k]

    return pl.pallas_call(
        kernel,
        in_specs=[smem()] + away() + near(slots - 1),
        out_specs=near(planes),
        out_shape=[pltpu.VMEM(shape, jnp.bfloat16)] * planes,
        scratch_shapes=[pltpu.VMEM((slots, *shape), jnp.bfloat16), pltpu.SemaphoreType.DMA],
        compiler_params=limit(12),
        cost_estimate=cost(1e9, 2e6),
        name="route",
    )(prefetch(here, plane), *pieces)


def add_up(groups):
    count, (rows, size) = len(groups[0]), groups[0][0].shape

    def kernel(*refs):
        for side in range(len(groups)):
            terms = refs[side * count : (side + 1) * count]
            total = terms[0][...].astype(jnp.float32)
            for ref in terms[1:]:
                total += ref[...].astype(jnp.float32)
            refs[-1][:, side * size : (side + 1) * size] = total.astype(jnp.bfloat16)

    return pl.pallas_call(
        kernel,
        in_specs=near(count * len(groups)),
        out_specs=near()[0],
        out_shape=pltpu.VMEM((rows, size * len(groups)), jnp.bfloat16),
        compiler_params=limit(12),
        cost_estimate=cost(1e9, 1e6),
        name="add_up",
    )(*[term for group in groups for term in group])


def lay_out(here, pieces):
    slots = len(pieces)
    share, size = pieces[0].shape

    def kernel(place, *refs):
        out, wide, sems = refs[slots:]

        def store(k):
            at = pl.ds(pl.multiple_of((place[0] ^ k) * size, size), size)
            return pltpu.make_async_copy(wide.at[k], out.at[:, at], sems.at[k])

        for k in range(slots):
            wide[k] = refs[k][...].astype(jnp.float32)
            store(k).start()
        for k in range(slots):
            store(k).wait()

    return pl.pallas_call(
        kernel,
        in_specs=[smem()] + near(slots),
        out_specs=away()[0],
        out_shape=jax.ShapeDtypeStruct((share, size * slots), jnp.float32),
        scratch_shapes=[
            pltpu.VMEM((slots, share, size), jnp.float32),
            pltpu.SemaphoreType.DMA((slots,)),
        ],
        compiler_params=limit(12),
        cost_estimate=cost(1e9, 4e6),
        name="lay_out",
    )(prefetch(here), *pieces)


def gather_slots(array):
    half = array.shape[1] // 2
    near_one, next_one = swap(array, "sp", 1), swap(array, "sp", 2)
    far = [swap(next_one[:, :half], "sp", 1), swap(near_one[:, half:], "sp", 2)]
    return [[array], [near_one], [next_one], far]


def direct_body(tokens, key_weight, queries, values, cotangent, log_decay):
    return direct_steps(tokens, key_weight, queries, values, cotangent, log_decay)


def direct_steps(tokens, key_weight, queries, values, cotangent, log_decay):
    here, member = lax.axis_index("sp"), lax.axis_index("dp")
    slots = lax.axis_size("sp")
    planes = lax.axis_size("dp") // 2
    plane, core = member // 2, member % 2
    seq_len, heads, key_width = queries.shape[1:]
    value_width = values.shape[3]
    rate = lax.dynamic_slice_in_dim(log_decay, here * heads, heads)
    cosine, sine = rotation(seq_len, key_width // 2)
    cosine, sine = cosine[:, 0], sine[:, 0]
    cosine = jnp.concatenate([cosine, cosine], axis=1)
    sine = jnp.concatenate([-sine, sine], axis=1)

    ring = [key_weight]
    for _ in range(1, planes):
        ring.append(step_planes(ring[-1]))
    shards = [(part, swap(part, "dp", 1)) for part in ring]

    cotans = [columns(cotangent[0], here ^ k, heads * value_width) for k in range(slots)]
    cotans = cotans[:1] + [swap(cotans[k], "sp", k) for k in range(1, slots)]
    token_slots = gather_slots(tokens[0])

    query = queries[0].reshape(seq_len, heads * key_width)
    value = values[0].reshape(seq_len, heads * value_width)
    grads, turned_grads, rotated, trailing = retention_first(
        here, rate, query, value, cosine, sine, cotans, key_width
    )

    total = weight_start(turned_grads[:-1], token_slots[:-1])
    sent = weight_end(core ^ 1, turned_grads[-1], token_slots[-1], total, jnp.bfloat16)
    received = swap(sent, "dp", 1)
    kept = weight_end(core, turned_grads[-1], token_slots[-1], total, jnp.float32)
    chunks = weight_pieces(here, slots, CHUNKS, kept, received)
    groups = []
    for pieces in chunks:
        came = [pieces[0]] + [swap(pieces[k], "sp", k) for k in range(1, slots)]
        terms = route(here, plane, planes, came)
        others = [swap(terms[k], "dp", 2 * k) for k in range(1, planes)]
        groups.append([terms[0]] + others)
    total = add_up(groups)
    gathered = [total] + [swap(total, "sp", k) for k in range(1, slots)]
    grad_weight = lay_out(here, gathered)

    returned = [grads[0]] + [swap(grads[k], "sp", k) for k in range(1, slots)]
    grad_tokens = token_gradient(here, plane, core, returned, shards)

    keys = key_projection(here, plane, core, token_slots, shards)
    grad_query, grad_value = retention_second(
        here, rate, rotated, value, cosine, sine, trailing, keys, cotans
    )
    grad_query = grad_query.reshape(queries.shape)
    grad_value = grad_value.reshape(values.shape)
    return (
        grad_tokens[None],
        grad_query,
        grad_value,
        grad_weight,
    )


def solution(mesh):
    slots, members = mesh.shape["sp"], mesh.shape["dp"]
    direct = members == 2 * slots and slots == 4
    return jax.shard_map(
        direct_body if direct else general_body,
        mesh=mesh,
        in_specs=(
            P("dp", "sp", None),
            P("dp", None),
            P("dp", None, "sp", None),
            P("dp", None, "sp", None),
            P("dp", "sp", None),
            P(),
        ),
        out_specs=(
            P("dp", "sp", None),
            P("dp", None, "sp", None),
            P("dp", None, "sp", None),
            P("dp", None),
        ),
        check_vma=False,
    )
```

```python
import jax
import jax.numpy as jnp
from jax import lax
from jax.experimental import pallas as pl
from jax.experimental.pallas import tpu as pltpu
from jax.sharding import PartitionSpec as P

BLOCK = 128


def product(form, left, right):
    return jnp.einsum(form, left, right, preferred_element_type=jnp.float32)


def rotation(seq_len, half):
    position = jnp.arange(seq_len, dtype=jnp.float32)
    frequency = 10000.0 ** (-jnp.arange(half, dtype=jnp.float32) / half)
    angle = position[:, None] * frequency[None, :]
    return (jnp.cos(angle)[:, None, :], jnp.sin(angle)[:, None, :])


def rotate(vectors, cosine, sine):
    half = vectors.shape[-1] // 2
    front, back = (vectors[..., :half], vectors[..., half:])
    return jnp.concatenate([front * cosine - back * sine, front * sine + back * cosine], axis=-1)


def unrotate(grads, cosine, sine):
    half = grads.shape[-1] // 2
    front, back = (grads[..., :half], grads[..., half:])
    return jnp.concatenate([front * cosine + back * sine, back * cosine - front * sine], axis=-1)


def retention_backward(query_rows, key_rows, value_rows, cotan_rows, head_decay):
    seq_len, heads_here, key_width = query_rows.shape
    nblocks = seq_len // BLOCK
    cosine, sine = rotation(seq_len, key_width // 2)
    factor = key_width ** (-0.5)
    rot_query = rotate(query_rows.astype(jnp.float32), cosine, sine).astype(jnp.bfloat16)
    rot_key = (rotate(key_rows.astype(jnp.float32), cosine, sine) * factor).astype(jnp.bfloat16)

    def blocks(array):
        return array.reshape(nblocks, BLOCK, heads_here, array.shape[-1])

    block_query, block_key = (blocks(rot_query), blocks(rot_key))
    block_value, block_cotan = (blocks(value_rows), blocks(cotan_rows))
    inside = jnp.arange(BLOCK, dtype=jnp.float32)
    offset = inside[:, None] - inside[None, :]
    within = jnp.where(
        offset[None] >= 0, jnp.exp(jnp.maximum(offset, 0.0)[None] * head_decay[:, None, None]), 0.0
    )
    rising = jnp.exp((inside + 1.0)[:, None] * head_decay[None, :])[None, :, :, None]
    falling = jnp.exp((BLOCK - 1.0 - inside)[:, None] * head_decay[None, :])[None, :, :, None]
    scores = (product("nihd,njhd->nhij", block_query, block_key) * within[None]).astype(
        jnp.bfloat16
    )
    mixing = (product("nihe,njhe->nhij", block_cotan, block_value) * within[None]).astype(
        jnp.bfloat16
    )
    decayed_queries = (block_query.astype(jnp.float32) * rising).astype(jnp.bfloat16)
    decayed_keys = (block_key.astype(jnp.float32) * falling).astype(jnp.bfloat16)
    block_states = product("nihd,nihe->nhde", decayed_keys, block_value)
    block_trails = product("nihd,nihe->nhde", decayed_queries, block_cotan)
    block_index = jnp.arange(nblocks, dtype=jnp.float32)
    spacing = block_index[:, None] - block_index[None, :] - 1.0
    earlier = jnp.where(
        spacing[None] >= 0,
        jnp.exp(jnp.maximum(spacing, 0.0)[None] * BLOCK * head_decay[:, None, None]),
        0.0,
    )
    later = jnp.transpose(earlier, (0, 2, 1))
    entering = jnp.einsum(
        "hnm,mhde->nhde", earlier, block_states, precision=lax.Precision.HIGHEST
    ).astype(jnp.bfloat16)
    trailing = jnp.einsum(
        "hnm,mhde->nhde", later, block_trails, precision=lax.Precision.HIGHEST
    ).astype(jnp.bfloat16)
    grad_rq = product("nhij,njhd->nihd", mixing, block_key) + rising * product(
        "nihe,nhde->nihd", block_cotan, entering
    )
    grad_rk = product("nhij,nihd->njhd", mixing, block_query) + falling * product(
        "nihe,nhde->nihd", block_value, trailing
    )
    grad_value = product("nhij,nihe->njhe", scores, block_cotan) + falling * product(
        "nihd,nhde->nihe", block_key, trailing
    )
    grad_rq = grad_rq.reshape(seq_len, heads_here, key_width)
    grad_rk = grad_rk.reshape(seq_len, heads_here, key_width)
    grad_query = unrotate(grad_rq, cosine, sine).astype(jnp.bfloat16)
    grad_key = (unrotate(grad_rk, cosine, sine) * factor).astype(jnp.bfloat16)
    grad_value = grad_value.reshape(seq_len, heads_here, -1).astype(jnp.bfloat16)
    return (grad_query, grad_key, grad_value)


def general_body(tokens, key_weight, queries, values, cotangent, log_decay):
    gathered = lax.all_gather(key_weight, "dp", axis=0, tiled=True)
    token_rows = tokens[0]
    key_proj = jnp.einsum(
        "td,qd->tq", token_rows, gathered, preferred_element_type=jnp.float32
    ).astype(jnp.bfloat16)
    head_keys, head_cotan = (
        lax.all_to_all(key_proj[None], "sp", split_axis=2, concat_axis=1, tiled=True),
        lax.all_to_all(cotangent, "sp", split_axis=2, concat_axis=1, tiled=True),
    )
    seq_len = head_keys.shape[1]
    heads_here = queries.shape[2]
    head_start = lax.axis_index("sp") * heads_here
    head_decay = lax.dynamic_slice_in_dim(log_decay, head_start, heads_here)
    grad_query, grad_key, grad_value = retention_backward(
        queries[0],
        head_keys[0].reshape(seq_len, heads_here, -1),
        values[0],
        head_cotan[0].reshape(seq_len, heads_here, -1),
        head_decay,
    )
    returned = lax.all_to_all(
        grad_key.reshape(1, seq_len, -1), "sp", split_axis=1, concat_axis=2, tiled=True
    )
    key_grads = returned[0]
    grad_tokens = jnp.dot(key_grads, gathered, preferred_element_type=jnp.float32).astype(
        jnp.bfloat16
    )
    width = key_grads.shape[1]
    count_dp = lax.axis_size("dp")
    count_sp = lax.axis_size("sp")
    share = width // (count_sp * count_dp)
    ordered = (
        key_grads.reshape(-1, count_dp, count_sp, share).transpose(0, 2, 1, 3).reshape(-1, width)
    )
    partial_grad = jnp.einsum("tq,td->qd", ordered, token_rows, preferred_element_type=jnp.float32)
    owned = lax.psum_scatter(partial_grad, ("sp", "dp"), scatter_dimension=0, tiled=True)
    weight_grad = lax.all_gather(owned, "sp", axis=0, tiled=True)
    return (grad_tokens[None], grad_query[None], grad_value[None], weight_grad)


INNER = 256
CHUNKS = 2


def swap(array, axis, bit):
    count = lax.axis_size(axis)
    return lax.ppermute(array, axis, [(i, i ^ bit) for i in range(count)])


def step_planes(array):
    count = lax.axis_size("dp")
    return lax.ppermute(array, "dp", [(i, (i + 2) % count) for i in range(count)])


def limit(mib):
    return pltpu.CompilerParams(vmem_limit_bytes=mib * 2**20)


def dot(left, right, left_dim, right_dim):
    return lax.dot_general(
        left, right, (((left_dim,), (right_dim,)), ((), ())), preferred_element_type=jnp.float32
    )


def columns(array, index, width):
    return lax.dynamic_slice_in_dim(array, index * width, width, axis=1)


def cost(flops, moved):
    return pl.CostEstimate(flops=int(flops), bytes_accessed=int(moved), transcendentals=0)


def spec(shape, index):
    return pl.BlockSpec(shape, index)


def decays(rate, size):
    rows = lax.broadcasted_iota(jnp.int32, (size, size), 0)
    cols = lax.broadcasted_iota(jnp.int32, (size, size), 1)
    gap = (rows - cols).astype(jnp.float32)
    within = jnp.where(gap >= 0, jnp.exp(jnp.maximum(gap, 0.0) * rate), 0.0)
    flipped = jnp.where(gap <= 0, jnp.exp(jnp.maximum(-gap, 0.0) * rate), 0.0)
    place = lax.broadcasted_iota(jnp.int32, (size, 1), 0).astype(jnp.float32)
    rising = jnp.exp((place + 1.0) * rate)
    falling = jnp.exp((size - 1.0 - place) * rate)
    whole = jnp.exp(jnp.full((1, 1), float(size), jnp.float32) * rate)
    return within, flipped, rising, falling, whole


def turn(block, cosine, sine):
    half = block.shape[-1] // 2
    return block * cosine + pltpu.roll(block, half, 1) * sine


def turn_back(block, cosine, sine):
    half = block.shape[-1] // 2
    return block * cosine - pltpu.roll(block, half, 1) * sine


def first_kernel(slots, rows, inner, factor):
    def kernel(*refs):
        place, rate_ref, query, value, cosine, sine = refs[:6]
        cotans = refs[6 : 6 + slots]
        outs = refs[6 + slots :]
        grads, turned_grads = outs[:slots], outs[slots : 2 * slots]
        rotated, trailing, cotan, whole_grad, flat_grad = outs[2 * slots :]
        here = place[0]
        rate = rate_ref[pl.program_id(0)]
        for k in range(slots):
            cotan[pl.ds((here ^ k) * rows, rows), :] = cotans[k][...]
        _, flipped, rising, falling, whole = decays(rate, inner)
        seq_len = query.shape[0]
        carry = jnp.zeros((query.shape[1], value.shape[1]), jnp.float32)
        for n in reversed(range(seq_len // inner)):
            at = slice(n * inner, (n + 1) * inner)
            cos, sin = cosine[at, :], sine[at, :]
            turned = turn(query[at, :].astype(jnp.float32), cos, sin).astype(jnp.bfloat16)
            rotated[at, :] = turned
            co, va = cotan[at, :], value[at, :]
            mix = (dot(va, co, 1, 1) * flipped).astype(jnp.bfloat16)
            trail = carry.astype(jnp.bfloat16)
            trailing[0, n] = trail
            grad = dot(mix, turned, 1, 0) + falling * dot(va, trail, 1, 1)
            grad = turn_back(grad, cos, sin) * factor
            whole_grad[at, :] = grad.astype(jnp.bfloat16)
            start = n * inner % rows
            flat_grad[n * inner // rows, :, start : start + inner] = grad.T.astype(jnp.bfloat16)
            decayed = (turned.astype(jnp.float32) * rising).astype(jnp.bfloat16)
            carry = carry * whole + dot(decayed, co, 0, 0)
        for k in range(slots):
            grads[k][...] = whole_grad[pl.ds((here ^ k) * rows, rows), :]
            turned_grads[k][...] = flat_grad[here ^ k]

    return kernel


def second_kernel(slots, rows, inner, factor):
    def kernel(*refs):
        place, rate_ref, rotated, value, cosine, sine, trailing, keys = refs[:8]
        cotans = refs[8 : 8 + slots]
        grad_query, grad_value, cotan, key = refs[8 + slots :]
        here = place[0]
        rate = rate_ref[pl.program_id(0)]
        for k in range(slots):
            at = pl.ds((here ^ k) * rows, rows)
            cotan[at, :] = cotans[k][...]
            key[at, :] = keys[k * rows : (k + 1) * rows, :]
        within, flipped, rising, falling, whole = decays(rate, inner)
        seq_len = rotated.shape[0]
        carry = jnp.zeros((rotated.shape[1], value.shape[1]), jnp.float32)
        for n in range(seq_len // inner):
            at = slice(n * inner, (n + 1) * inner)
            cos, sin = cosine[at, :], sine[at, :]
            rk = (turn(key[at, :].astype(jnp.float32), cos, sin) * factor).astype(jnp.bfloat16)
            rq, co, va = rotated[at, :], cotan[at, :], value[at, :]
            score = (dot(rk, rq, 1, 1) * flipped).astype(jnp.bfloat16)
            entering = carry.astype(jnp.bfloat16)
            mix = (dot(co, va, 1, 1) * within).astype(jnp.bfloat16)
            grad = dot(mix, rk, 1, 0) + rising * dot(co, entering, 1, 1)
            grad_query[at, :] = turn_back(grad, cos, sin).astype(jnp.bfloat16)
            grad_value[at, :] = (
                dot(score, co, 1, 0) + falling * dot(rk, trailing[0, n], 1, 0)
            ).astype(jnp.bfloat16)
            decayed = (rk.astype(jnp.float32) * falling).astype(jnp.bfloat16)
            carry = carry * whole + dot(decayed, va, 0, 0)

    return kernel


def prefetch(*values):
    return jnp.stack([jnp.asarray(v, jnp.int32) for v in values])


def near(count=1):
    return [pl.BlockSpec(memory_space=pltpu.VMEM)] * count


def away(count=1):
    return [pl.BlockSpec(memory_space=pltpu.HBM)] * count


def smem():
    return pl.BlockSpec(memory_space=pltpu.SMEM)


def retention_first(here, rate, query, value, cosine, sine, cotans, key_width):
    slots = len(cotans)
    seq_len, query_width = query.shape
    heads = query_width // key_width
    value_width = value.shape[1] // heads
    rows = cotans[0].shape[0]
    inner = min(INNER, rows)
    nblocks = seq_len // inner
    half = jnp.bfloat16
    full = spec((seq_len, key_width), lambda h: (0, 0))
    head = spec((seq_len, key_width), lambda h: (0, h))
    outs = [pltpu.HBM((rows, query_width), half)] * slots
    outs += [pltpu.VMEM((query_width, rows), half)] * slots
    outs += [
        pltpu.HBM((seq_len, query_width), half),
        pltpu.HBM((heads, nblocks, key_width, value_width), half),
    ]
    result = pl.pallas_call(
        first_kernel(slots, rows, inner, key_width**-0.5),
        grid=(heads,),
        in_specs=[smem(), smem(), head, spec((seq_len, value_width), lambda h: (0, h)), full, full]
        + [spec((rows, value_width), lambda h: (0, h))] * slots,
        out_specs=[spec((rows, key_width), lambda h: (0, h))] * slots
        + [spec((key_width, rows), lambda h: (h, 0))] * slots
        + [
            head,
            spec((1, nblocks, key_width, value_width), lambda h: (h, 0, 0, 0)),
        ],
        out_shape=outs,
        scratch_shapes=[
            pltpu.VMEM((seq_len, value_width), half),
            pltpu.VMEM((seq_len, key_width), half),
            pltpu.VMEM((slots, key_width, rows), half),
        ],
        compiler_params=limit(16),
        cost_estimate=cost(6e9, 10e6),
        name="retention_first",
    )(prefetch(here), rate, query, value, cosine, sine, *cotans)
    return list(result[:slots]), list(result[slots : 2 * slots]), *result[2 * slots :]


def retention_second(here, rate, rotated, value, cosine, sine, trailing, keys, cotans):
    slots = len(cotans)
    heads, nblocks, key_width, value_width = trailing.shape
    seq_len = rotated.shape[0]
    inner = seq_len // nblocks
    rows = cotans[0].shape[0]
    half = jnp.bfloat16
    full = spec((seq_len, key_width), lambda h: (0, 0))
    head = spec((seq_len, key_width), lambda h: (0, h))
    wide = spec((seq_len, value_width), lambda h: (0, h))
    return pl.pallas_call(
        second_kernel(slots, rows, inner, key_width**-0.5),
        grid=(heads,),
        in_specs=[
            smem(),
            smem(),
            head,
            wide,
            full,
            full,
            spec((1, nblocks, key_width, value_width), lambda h: (h, 0, 0, 0)),
            spec((slots * rows, key_width), lambda h: (0, h)),
        ]
        + [spec((rows, value_width), lambda h: (0, h))] * slots,
        out_specs=[head, wide],
        out_shape=[
            pltpu.HBM(rotated.shape, half),
            pltpu.HBM(value.shape, half),
        ],
        scratch_shapes=[
            pltpu.VMEM((seq_len, value_width), half),
            pltpu.VMEM((seq_len, key_width), half),
        ],
        compiler_params=limit(16),
        cost_estimate=cost(6e9, 14e6),
        name="retention_second",
    )(prefetch(here), rate, rotated, value, cosine, sine, trailing, keys, *cotans)


def halves(tokens):
    width = sum(part.shape[1] for part in tokens[0])
    found, place = ([], []), 0
    for k, parts in enumerate(tokens):
        for at, part in place_parts(parts):
            for piece in range(2 * part.shape[1] // width):
                found[2 * at // width + piece].append((k, place, piece))
            place += 1
    return found


def key_projection(here, plane, core, tokens, shards):
    slots = len(tokens)
    planes = len(shards)
    parts = [part for slot in tokens for part in slot]
    loads = halves(tokens)
    rows, width = tokens[0][0].shape[0], sum(part.shape[1] for part in tokens[0])
    share = shards[0][0].shape[0]
    half = width // 2

    def kernel(*refs):
        place = refs[0]
        token_refs = refs[1 : 1 + len(parts)]
        shard_refs = refs[1 + len(parts) : 1 + len(parts) + 2 * planes]
        out, weight, token, total, sems = refs[1 + len(parts) + 2 * planes :]
        slot, own = place[0], place[1]

        def weight_copy(r, side, at):
            return pltpu.make_async_copy(
                shard_refs[2 * r + side].at[:, at * half : (at + 1) * half],
                weight.at[at, pl.ds(pl.multiple_of((own ^ side) * share, share), share)],
                sems.at[at, slots + side],
            )

        def token_copy(at, k, index, piece):
            return pltpu.make_async_copy(
                token_refs[index].at[:, piece * half : (piece + 1) * half],
                token.at[at, k * rows : (k + 1) * rows],
                sems.at[at, k],
            )

        for at in range(2):
            for r in range(planes):

                @pl.when(slot == r)
                def _():
                    for side in range(2):
                        weight_copy(r, side, at).start()

            for k, index, piece in loads[at]:
                token_copy(at, k, index, piece).start()
        for at in range(2):
            for side in range(2):
                weight_copy(0, side, at).wait()
            for k, index, piece in loads[at]:
                token_copy(at, k, index, piece).wait()
            term = dot(token[at], weight[at], 1, 1)
            if at == 0:
                total[...] = term
            else:
                out[...] = (total[...] + term).astype(jnp.bfloat16)

    far = len(tokens[-1])
    return pl.pallas_call(
        kernel,
        in_specs=[smem()] + away(len(parts) - far) + near(far) + away(2 * planes),
        out_specs=near()[0],
        out_shape=pltpu.VMEM((slots * rows, 2 * share), jnp.bfloat16),
        scratch_shapes=[
            pltpu.VMEM((2, 2 * share, half), jnp.bfloat16),
            pltpu.VMEM((2, slots * rows, half), jnp.bfloat16),
            pltpu.VMEM((slots * rows, 2 * share), jnp.float32),
            pltpu.SemaphoreType.DMA((2, slots + 2)),
        ],
        compiler_params=limit(20),
        cost_estimate=cost(4e9, 8e6),
        name="key_projection",
    )(
        prefetch((plane - here) % planes, core),
        *parts,
        *[part for pair in shards for part in pair],
    )


def token_gradient(here, plane, core, grads, shards, flats, heads):
    slots = len(grads)
    planes = len(shards)
    rows = grads[0].shape[0]
    share, width = shards[0][0].shape
    seq_len = flats[0].shape[0]
    block = seq_len // planes
    widths = [flat.shape[1] // heads for flat in flats]
    count = len(flats)

    def kernel(*refs):
        place = refs[0]
        grad_refs = refs[1 : 1 + slots]
        shard_refs = refs[1 + slots : 1 + slots + 2 * planes]
        rest = refs[1 + slots + 2 * planes :]
        flat_refs, out, open_refs = rest[:count], rest[count], rest[count + 1 : 2 * count + 1]
        grad, weight, total = rest[2 * count + 1 : 2 * count + 4]
        flat_blocks, open_blocks = rest[2 * count + 4 : 3 * count + 4], rest[3 * count + 4 : -2]
        sems, flat_sems = rest[-2:]
        own = place[2]

        def grad_copy(k):
            return pltpu.make_async_copy(grad_refs[k], grad.at[k], sems.at[2 * planes + k])

        def shard_copy(r, side):
            return pltpu.make_async_copy(
                shard_refs[2 * r + side], weight.at[r, own ^ side], sems.at[2 * r + side]
            )

        def flat_copy(i, r):
            part = flat_refs[i].at[r * block : (r + 1) * block]
            return pltpu.make_async_copy(part, flat_blocks[i].at[r], flat_sems.at[0, i, r])

        def open_copy(i, r):
            part = open_refs[i].at[r * block : (r + 1) * block]
            return pltpu.make_async_copy(open_blocks[i].at[r], part, flat_sems.at[1, i, r])

        for i in range(count):
            flat_copy(i, 0).start()
        for k in range(slots):
            grad_copy(k).start()
        for r in range(planes):
            for side in range(2):
                shard_copy(r, side).start()
            if r + 1 < planes:
                for i in range(count):
                    flat_copy(i, r + 1).start()
        for k in range(slots):
            grad_copy(k).wait()
        for r in range(planes):
            for i in range(count):
                flat_copy(i, r).wait()
                opened = flat_blocks[i][r].reshape(block, heads, widths[i])
                open_blocks[i][r] = opened
                open_copy(i, r).start()
            k = ((place[1] + planes - r) % planes) ^ place[0]
            for side in range(2):
                shard_copy(r, side).wait()
            piece = grad[k]
            term = dot(piece[:, :share], weight[r, 0], 1, 0)
            term += dot(piece[:, share:], weight[r, 1], 1, 0)
            if r == 0:
                total[...] = term
            elif r < planes - 1:
                total[...] += term
            else:
                out[...] = (total[...] + term).astype(jnp.bfloat16)
        for r in range(planes):
            for i in range(count):
                open_copy(i, r).wait()

    return pl.pallas_call(
        kernel,
        in_specs=[smem()] + away(slots + 2 * planes + count),
        out_specs=near() + away(count),
        out_shape=[jax.ShapeDtypeStruct((rows, width), jnp.bfloat16)]
        + [jax.ShapeDtypeStruct((seq_len, heads, size), jnp.bfloat16) for size in widths],
        scratch_shapes=[
            pltpu.VMEM((slots, rows, 2 * share), jnp.bfloat16),
            pltpu.VMEM((planes, 2, share, width), jnp.bfloat16),
            pltpu.VMEM((rows, width), jnp.float32),
        ]
        + [pltpu.VMEM((planes, block, heads * size), jnp.bfloat16) for size in widths]
        + [pltpu.VMEM((planes, block, heads, size), jnp.bfloat16) for size in widths]
        + [
            pltpu.SemaphoreType.DMA((2 * planes + slots,)),
            pltpu.SemaphoreType.DMA((2, count, planes)),
        ],
        compiler_params=limit(32),
        cost_estimate=cost(5e9, 17e6),
        name="token_gradient",
    )(prefetch(here, plane, core), *grads, *[part for pair in shards for part in pair], *flats)


def place_parts(parts):
    at, placed = 0, []
    for part in parts:
        placed.append((at, part))
        at += part.shape[1]
    return placed


def weight_start(grads, tokens):
    slots = len(tokens)
    features, rows = grads[0].shape
    parts = [part for slot in tokens for part in slot]
    loads = halves(tokens)
    width = sum(part.shape[1] for part in tokens[0])
    half = width // 2

    def kernel(*refs):
        grad_refs, token_refs = refs[:slots], refs[slots : slots + len(parts)]
        out, token, sems = refs[slots + len(parts) :]

        def fetch(at, k, index, piece):
            return pltpu.make_async_copy(
                token_refs[index].at[:, piece * half : (piece + 1) * half],
                token.at[at, k],
                sems.at[at, k],
            )

        for at in range(2):
            for load in loads[at]:
                fetch(at, *load).start()
        for at in range(2):
            for load in loads[at]:
                fetch(at, *load).wait()
            total = dot(grad_refs[0][...], token[at, 0], 1, 0)
            for k in range(1, slots):
                total += dot(grad_refs[k][...], token[at, k], 1, 0)
            out[:, at * half : (at + 1) * half] = total

    return pl.pallas_call(
        kernel,
        in_specs=near(slots) + away(len(parts)),
        out_specs=near()[0],
        out_shape=pltpu.VMEM((features, width), jnp.float32),
        scratch_shapes=[
            pltpu.VMEM((2, slots, rows, half), jnp.bfloat16),
            pltpu.SemaphoreType.DMA((2, slots)),
        ],
        compiler_params=limit(20),
        cost_estimate=cost(4e9, 6e6),
        name="weight_start",
    )(*grads, *parts)


def weight_end(side, grad, tokens, total, kind):
    features, width = total.shape
    share = features // 2

    def kernel(place, grad_ref, *refs):
        token_refs, (so_far, out) = refs[: len(tokens)], refs[len(tokens) :]
        rows = pl.ds(pl.multiple_of(place[0] * share, share), share)
        for (at, part), ref in zip(place_parts(tokens), token_refs):
            to = slice(at, at + part.shape[1])
            term = dot(grad_ref[rows, :], ref[...], 1, 0)
            out[:, to] = (so_far[rows, to] + term).astype(kind)

    return pl.pallas_call(
        kernel,
        in_specs=[smem()] + near(2 + len(tokens)),
        out_specs=near()[0],
        out_shape=pltpu.VMEM((share, width), kind),
        compiler_params=limit(20),
        cost_estimate=cost(2e9, 6e6),
        name="weight_end",
    )(prefetch(side), grad, *tokens, total)


def weight_pieces(here, slots, chunks, kept, received):
    share, width = kept.shape
    tile = width // slots
    size = tile // chunks

    def kernel(place, own, other, *outs):
        for k in range(slots):
            for chunk in range(chunks):
                start = pl.multiple_of((place[0] ^ k) * tile + chunk * size, size)
                at = pl.ds(start, size)
                total = own[:, at] + other[:, at].astype(jnp.float32)
                outs[chunk * slots + k][...] = total.astype(jnp.bfloat16)

    result = pl.pallas_call(
        kernel,
        in_specs=[smem()] + near(2),
        out_specs=near(slots * chunks),
        out_shape=([pltpu.HBM((share, size), jnp.bfloat16)] + [pltpu.VMEM((share, size), jnp.bfloat16)] * (slots - 1)) * chunks,
        compiler_params=limit(12),
        cost_estimate=cost(2e9, 6e6),
        name="weight_pieces",
    )(prefetch(here), kept, received)
    return [result[chunk * slots : (chunk + 1) * slots] for chunk in range(chunks)]


def route(here, plane, planes, pieces):
    slots = len(pieces)
    shape = pieces[0].shape

    def kernel(place, *refs):
        outs, (stack, sem) = refs[slots:-2], refs[-2:]
        own = pltpu.make_async_copy(refs[0], stack.at[0], sem)
        own.start()
        for k in range(1, slots):
            stack[k] = refs[k][...]
        own.wait()
        for k in range(planes):
            outs[k][...] = stack[place[0] ^ place[1] ^ k]

    return pl.pallas_call(
        kernel,
        in_specs=[smem()] + away() + near(slots - 1),
        out_specs=near(planes),
        out_shape=[pltpu.VMEM(shape, jnp.bfloat16)] * planes,
        scratch_shapes=[pltpu.VMEM((slots, *shape), jnp.bfloat16), pltpu.SemaphoreType.DMA],
        compiler_params=limit(12),
        cost_estimate=cost(1e9, 2e6),
        name="route",
    )(prefetch(here, plane), *pieces)


def add_up(groups):
    count, (rows, size) = len(groups[0]), groups[0][0].shape

    def kernel(*refs):
        for side in range(len(groups)):
            terms = refs[side * count : (side + 1) * count]
            total = terms[0][...].astype(jnp.float32)
            for ref in terms[1:]:
                total += ref[...].astype(jnp.float32)
            refs[-1][:, side * size : (side + 1) * size] = total.astype(jnp.bfloat16)

    return pl.pallas_call(
        kernel,
        in_specs=near(count * len(groups)),
        out_specs=near()[0],
        out_shape=pltpu.VMEM((rows, size * len(groups)), jnp.bfloat16),
        compiler_params=limit(12),
        cost_estimate=cost(1e9, 1e6),
        name="add_up",
    )(*[term for group in groups for term in group])


def lay_out(here, pieces):
    slots = len(pieces)
    share, size = pieces[0].shape

    def kernel(place, *refs):
        out, wide, sems = refs[slots:]

        def store(k):
            at = pl.ds(pl.multiple_of((place[0] ^ k) * size, size), size)
            return pltpu.make_async_copy(wide.at[k], out.at[:, at], sems.at[k])

        for k in range(slots):
            wide[k] = refs[k][...].astype(jnp.float32)
            store(k).start()
        for k in range(slots):
            store(k).wait()

    return pl.pallas_call(
        kernel,
        in_specs=[smem()] + near(slots),
        out_specs=away()[0],
        out_shape=jax.ShapeDtypeStruct((share, size * slots), jnp.float32),
        scratch_shapes=[
            pltpu.VMEM((slots, share, size), jnp.float32),
            pltpu.SemaphoreType.DMA((slots,)),
        ],
        compiler_params=limit(12),
        cost_estimate=cost(1e9, 4e6),
        name="lay_out",
    )(prefetch(here), *pieces)


def gather_slots(array):
    half = array.shape[1] // 2
    near_one, next_one = swap(array, "sp", 1), swap(array, "sp", 2)
    far = [swap(next_one[:, :half], "sp", 1), swap(near_one[:, half:], "sp", 2)]
    return [[array], [near_one], [next_one], far]


def direct_body(tokens, key_weight, queries, values, cotangent, log_decay):
    return direct_steps(tokens, key_weight, queries, values, cotangent, log_decay)


def direct_steps(tokens, key_weight, queries, values, cotangent, log_decay):
    here, member = lax.axis_index("sp"), lax.axis_index("dp")
    slots = lax.axis_size("sp")
    planes = lax.axis_size("dp") // 2
    plane, core = member // 2, member % 2
    seq_len, heads, key_width = queries.shape[1:]
    value_width = values.shape[3]
    rate = lax.dynamic_slice_in_dim(log_decay, here * heads, heads)
    cosine, sine = rotation(seq_len, key_width // 2)
    cosine, sine = cosine[:, 0], sine[:, 0]
    cosine = jnp.concatenate([cosine, cosine], axis=1)
    sine = jnp.concatenate([-sine, sine], axis=1)

    ring = [key_weight]
    for _ in range(1, planes):
        ring.append(step_planes(ring[-1]))
    shards = [(part, swap(part, "dp", 1)) for part in ring]

    cotans = [columns(cotangent[0], here ^ k, heads * value_width) for k in range(slots)]
    cotans = cotans[:1] + [swap(cotans[k], "sp", k) for k in range(1, slots)]
    token_slots = gather_slots(tokens[0])

    query = queries[0].reshape(seq_len, heads * key_width)
    value = values[0].reshape(seq_len, heads * value_width)
    grads, turned_grads, rotated, trailing = retention_first(
        here, rate, query, value, cosine, sine, cotans, key_width
    )

    total = weight_start(turned_grads[:-1], token_slots[:-1])
    sent = weight_end(core ^ 1, turned_grads[-1], token_slots[-1], total, jnp.bfloat16)
    received = swap(sent, "dp", 1)
    kept = weight_end(core, turned_grads[-1], token_slots[-1], total, jnp.float32)
    chunks = weight_pieces(here, slots, CHUNKS, kept, received)
    groups = []
    for pieces in chunks:
        came = [pieces[0]] + [swap(pieces[k], "sp", k) for k in range(1, slots)]
        terms = route(here, plane, planes, came)
        others = [swap(terms[k], "dp", 2 * k) for k in range(1, planes)]
        groups.append([terms[0]] + others)
    total = add_up(groups)
    gathered = [total] + [swap(total, "sp", k) for k in range(1, slots)]
    grad_weight = lay_out(here, gathered)

    returned = [grads[0]] + [swap(grads[k], "sp", k) for k in range(1, slots)]
    keys = key_projection(here, plane, core, token_slots, shards)
    grad_query, grad_value = retention_second(
        here, rate, rotated, value, cosine, sine, trailing, keys, cotans
    )
    grad_tokens, grad_query, grad_value = token_gradient(
        here, plane, core, returned, shards, [grad_query, grad_value], heads
    )
    grad_query, grad_value = grad_query[None], grad_value[None]
    return (
        grad_tokens[None],
        grad_query,
        grad_value,
        grad_weight,
    )


def solution(mesh):
    slots, members = mesh.shape["sp"], mesh.shape["dp"]
    direct = members == 2 * slots and slots == 4
    return jax.shard_map(
        direct_body if direct else general_body,
        mesh=mesh,
        in_specs=(
            P("dp", "sp", None),
            P("dp", None),
            P("dp", None, "sp", None),
            P("dp", None, "sp", None),
            P("dp", "sp", None),
            P(),
        ),
        out_specs=(
            P("dp", "sp", None),
            P("dp", None, "sp", None),
            P("dp", None, "sp", None),
            P("dp", None),
        ),
        check_vma=False,
    )
```
